32 devices in a mesh: fs: 8 (over z, x), tp: 4 (over y, core).
Axes of the slice: x: 2, y: 2, z: 4, core: 2. Of those that a mesh axis runs over, the one named last changes fastest.
Arguments:
- prompt_tokens: bfloat16 [6144, 2048], P('fs', 'tp'), may hold values from -6 to 6
- norm_gain: float32 [2048], P('fs'), may hold values from 0.1 to 1.9
- up_master: float32 [2048, 4096], P('fs', 'tp'), may hold values from -6 to 6
- down_master: float32 [2048, 4096], P('fs', 'tp'), may hold values from -6 to 6
Outputs:
- serve_up: bfloat16 [2048, 4096], P(None, 'tp')
- serve_down: bfloat16 [2048, 4096], P(None, 'tp')
- mixed: bfloat16 [6144, 2048], P('fs', 'tp')
The draws below stay inside these ranges and needn't reach their ends.
All inputs are finite; a program needn't handle non-finite values.
Results may differ from the reference program's by a relative error of at most 0.009.
Values may be sent and summed in bfloat16 or wider, within the bound.
A program may use at most 64 MiB of HBM per device.

```python
import jax
import jax.numpy as jnp
from jax import lax

D = 2048
FF = 4096
TOK_DEV = 768
TOKENS = 6144
N_FS = 8
N_TP = 4


def steps_of(own_key, extent, shards, low, high):
    level = 1.0
    for dim, shards_of in shards:
        heights = jax.random.uniform(jax.random.fold_in(jax.random.fold_in(own_key, 6), dim), (shards_of,), jnp.float32, low / len(shards), high / len(shards))
        level = level * jnp.repeat(jnp.exp(heights), extent[dim] // shards_of).reshape((-1,) + (1,) * (len(extent) - 1 - dim))
    return level


def centred(own_key, shape, deviation, most, split=(), held_as=jnp.bfloat16):
    values = jax.random.normal(own_key, shape, jnp.float32) * deviation
    if len(split) > 0:
        values = steps_of(own_key, shape, split, -0.22, 0.18) * values
    return jnp.clip(values, min=-most, max=most).astype(held_as)


def setup_inputs(seed: int = 0) -> dict:
    arg_keys = jax.random.split(jax.random.key(seed), 5)
    prompt_tokens = centred(arg_keys[0], (TOKENS, D), 1.0, 6.0, ((0, 8), (1, 4)))
    norm_gain = jnp.clip(1.0 + 0.18 * jax.random.normal(arg_keys[1], (D,), jnp.float32), 0.1, 1.9)
    up_master = centred(arg_keys[2], (D, FF), 1.0, 6.0, ((0, 8), (1, 4)), jnp.float32)
    down_master = centred(arg_keys[3], (D, FF), 1.0, 6.0, ((0, 8), (1, 4)), jnp.float32)
    return dict(prompt_tokens=prompt_tokens, norm_gain=norm_gain, up_master=up_master, down_master=down_master)


def reference(prompt_tokens, norm_gain, up_master, down_master):
    serve_up = (norm_gain[:, None] * up_master).astype(jnp.bfloat16)
    serve_down = down_master.astype(jnp.bfloat16)
    group = FF // N_TP
    blocks = prompt_tokens.reshape(N_FS, TOK_DEV, D)

    def one_block(block):
        wide = block.astype(jnp.float32)
        normed = (wide * lax.rsqrt(lax.optimization_barrier(jnp.mean(wide * wide, axis=1, keepdims=True)) + 1e-05)).astype(jnp.bfloat16)
        hidden = jnp.dot(normed, serve_up, preferred_element_type=jnp.float32) * D ** (-0.5)
        act = jnp.square(jax.nn.relu(hidden)).astype(jnp.bfloat16)
        total = jnp.zeros((TOK_DEV, D), jnp.float32)
        for index in range(N_TP):
            act_part = act[:, index * group:(index + 1) * group]
            down_part = serve_down[:, index * group:(index + 1) * group]
            partial_value = lax.dot_general(act_part, down_part, (((1,), (1,)), ((), ())), preferred_element_type=jnp.float32) * FF ** (-0.5)
            total = total + partial_value.astype(jnp.bfloat16).astype(jnp.float32)
        return total.astype(jnp.bfloat16)
    mixed = lax.map(one_block, blocks).reshape(TOKENS, D)
    return (serve_up, serve_down, mixed)
```

```python
import functools

import jax
import jax.numpy as jnp
from jax import lax
from jax.experimental import pallas as pl
from jax.experimental.pallas import tpu as pltpu
from jax.sharding import PartitionSpec as P

MESH = pl.DeviceIdType.MESH
LANES = 128


def plain(prompt_tokens, norm_gain, up_master, down_master):
    up_folded = (norm_gain[:, None] * up_master).astype(jnp.bfloat16)
    down_cast = down_master.astype(jnp.bfloat16)
    whole = lax.all_gather(prompt_tokens, "tp", axis=1, tiled=True)
    width = whole.shape[1]
    hidden_units = up_master.shape[1] * lax.axis_size("tp")
    wide = whole.astype(jnp.float32)
    normed = (wide * lax.rsqrt(jnp.mean(wide * wide, axis=1, keepdims=True) + 1e-05)).astype(
        jnp.bfloat16
    )
    contract = (((1,), (1,)), ((), ()))
    serve_up, serve_down = (
        lax.all_gather(up_folded, "fs", axis=0, tiled=True),
        lax.all_gather(down_cast, "fs", axis=0, tiled=True),
    )
    hidden = jnp.dot(normed, serve_up, preferred_element_type=jnp.float32)
    act = jnp.square(jax.nn.relu(hidden * width ** (-0.5))).astype(jnp.bfloat16)
    product = lax.dot_general(act, serve_down, contract, preferred_element_type=jnp.float32)
    partial_value = (product * hidden_units ** (-0.5)).astype(jnp.bfloat16)
    mixed = lax.psum_scatter(partial_value, "tp", scatter_dimension=1, tiled=True)
    return (serve_up, serve_down, mixed)


def kernel(line, pieces, tok, gain_hbm, up_hbm, down_hbm, wu, wd, mixed,
           xt, xn, act, part, pbuf, psum, rin_p, rin_y,
           w_send, w_recv, t_send, t_recv, a_send, a_recv, b_send, b_recv, c_send, c_recv,
           l_sem, up, down, gain, d_sem):
    T, dl = tok.shape
    r, F = up_hbm.shape
    D = wu.shape[0]
    tp = lax.axis_index("tp")
    fs = lax.axis_index("fs")
    z, x = fs // 2, fs % 2
    core, chip = tp % 2, tp // 2
    partner = tp + 1 - 2 * core
    mirror = (tp + 2) % 4
    diag = (partner + 2) % 4
    has_up, has_dn = z < line - 1, z > 0
    inner = has_up & has_dn
    outer = jnp.logical_not(inner)
    low = z < line / 2
    W = (wu, wd)
    nb = dl // LANES
    per = r // LANES
    half = T // 2
    zdev = ((fs + 2, tp), (fs - 2, tp), (fs + 1 - 2 * x, tp))

    barrier = pltpu.get_barrier_semaphore()

    def greet(dev):
        pl.semaphore_signal(barrier, inc=1, device_id=dev, device_id_type=MESH)

    greet(zdev[2])
    pl.when(has_up)(lambda: greet(zdev[0]))
    pl.when(has_dn)(lambda: greet(zdev[1]))
    for other in (mirror, diag, partner):
        greet((fs, other))

    loads = [pltpu.make_async_copy(gain_hbm, gain, d_sem.at[0]),
             pltpu.make_async_copy(up_hbm, up, d_sem.at[1]),
             pltpu.make_async_copy(down_hbm, down, d_sem.at[2])]
    own_tok = pltpu.make_async_copy(tok, xt.at[tp], l_sem)
    for load in loads + [own_tok]:
        load.start()

    base = pl.multiple_of(fs * r, r)
    loads[0].wait()
    loads[1].wait()
    for i in range(per):
        rows = slice(i * LANES, (i + 1) * LANES)
        g = jnp.transpose(jnp.broadcast_to(gain[:, rows], (LANES, LANES)))
        for c in range(F // LANES):
            cols = slice(c * LANES, (c + 1) * LANES)
            wu[pl.ds(base + i * LANES, LANES), cols] = (g * up[rows, cols]).astype(jnp.bfloat16)
    loads[2].wait()
    wd[pl.ds(base, r), :] = down[...].astype(jnp.bfloat16)
    links = 4 + has_up.astype(jnp.int32) + has_dn.astype(jnp.int32)
    pl.semaphore_wait(barrier, links)

    def piece(a, s, p, way):
        start, size = pieces[p][0], pieces[p][1]
        ref = W[a].at[pl.ds(pl.multiple_of(s * r + start, 8), size), :]
        return pltpu.make_async_remote_copy(
            src_ref=ref, dst_ref=ref, send_sem=w_send.at[way, a, s, p],
            recv_sem=w_recv.at[a, s, p], device_id=zdev[way], device_id_type=MESH)

    def tok_copy(src, k, slot, to):
        return pltpu.make_async_remote_copy(
            src_ref=src, dst_ref=xt.at[k], send_sem=t_send.at[slot], recv_sem=t_recv.at[k],
            device_id=(fs, to), device_id_type=MESH)

    one = [p for p in range(len(pieces)) if pieces[p][2] == 1]
    two = [p for p in range(len(pieces)) if pieces[p][2] == 2]
    early = [p for p in one if pieces[p][0] < r - LANES]
    late = [p for p in one if p not in early]

    def start(d):
        d.start()

    def wait_send(d):
        d.wait_send()

    def own_z(a, do, up_cond, dn_cond):
        for p in one + two:
            pl.when(up_cond)(lambda: do(piece(a, fs, p, 0)))
            pl.when(dn_cond)(lambda: do(piece(a, fs, p, 1)))

    def own_x(a, do, which):
        for p in which:
            do(piece(a, fs, p, 2))

    xs = fs + 1 - 2 * x

    def cross(a, do, wait):
        for p in two:
            if wait:
                piece(a, xs, p, 2).wait_recv()
            pl.when(has_up)(lambda: do(piece(a, xs, p, 0)))
            pl.when(has_dn)(lambda: do(piece(a, xs, p, 1)))

    def near(i, k):
        return (abs(k - i), -k if i < line / 2 else k)

    def chip_of(k):
        return (2 * k * per // nb) // 2

    def pick(table):
        got = jnp.int32(0)
        for i in range(line):
            for y in range(2):
                got = got + jnp.where((z == i) & (chip == y), jnp.int32(table(i, y)), jnp.int32(0))
        return got

    order_a = [pick(lambda i, y: sorted(range(line), key=lambda k: near(i, k))[q])
               for q in range(line)]
    order_b = [pick(lambda i, y: sorted(range(line), key=lambda k: (
        k != i, chip_of(k) == y, near(i, k)))[q]) for q in range(line)]
    own_late = inner & (pick(lambda i, y: int(chip_of(i) == y)) == 1)

    def relay(a, zz, do, wait, ones=(), twos=()):
        onward_up = (zz < z) & has_up
        onward_dn = (zz > z) & has_dn
        same, cross_s = zz * 2 + x, zz * 2 + 1 - x
        for p in ones:
            if wait:
                piece(a, same, p, 2).wait_recv()
            pl.when(onward_up)(lambda: do(piece(a, same, p, 0)))
            pl.when(onward_dn)(lambda: do(piece(a, same, p, 1)))
            do(piece(a, same, p, 2))
        for p in twos:
            for s in (same, cross_s):
                if wait:
                    piece(a, s, p, 2).wait_recv()
                pl.when(onward_up)(lambda: do(piece(a, s, p, 0)))
                pl.when(onward_dn)(lambda: do(piece(a, s, p, 1)))

    own_x(0, start, two)
    own_z(0, start, has_up, has_dn)
    own_x(1, start, two)
    own_x(0, start, one)
    own_tok.wait()
    tok_copy(xt.at[tp], tp, 0, mirror).start()
    tok_copy(xt.at[tp], tp, 1, partner).start()
    cross(0, start, True)
    cross(1, start, True)
    own_z(1, start, outer & has_up, outer & has_dn)
    for idx in range(1, line):
        relay(0, order_a[idx], start, True, one, two)
        if idx == line - 2:
            own_z(1, start, inner & low, inner & jnp.logical_not(low))
            pl.when(outer)(lambda: own_x(1, start, one))
    pl.when(inner)(lambda: own_x(1, start, one))
    soon = inner & jnp.logical_not(own_late)
    own_z(1, start, soon & jnp.logical_not(low), soon & low)

    tok_copy(xt.at[mirror], mirror, 0, mirror).wait_recv()
    tok_copy(xt.at[mirror], mirror, 2, partner).start()
    tok_copy(xt.at[partner], partner, 1, partner).wait_recv()
    tok_copy(xt.at[diag], diag, 1, partner).wait_recv()
    block = 64

    def norm(i, carry):
        rows = pl.ds(pl.multiple_of(i * block, block), block)
        wide = [xt[k, rows, :].astype(jnp.float32) for k in range(4)]
        sq = wide[0] * wide[0]
        for k in range(1, 4):
            sq = sq + wide[k] * wide[k]
        inv = lax.rsqrt(jnp.sum(sq, axis=1, keepdims=True) * (1.0 / D) + 1e-05)
        for k in range(4):
            xn[rows, k * dl:(k + 1) * dl] = (wide[k] * inv).astype(jnp.bfloat16)
        return carry

    lax.fori_loop(0, T // block, norm, 0)

    relay(1, order_b[1], start, True, one, two)
    for q in range(line):
        for p in one:
            piece(0, order_a[q] * 2 + 1 - x, p, 2).wait_recv()

    mrows = 2 * LANES

    def first(i, carry):
        rows = pl.ds(pl.multiple_of(i * mrows, mrows), mrows)
        hidden = jnp.dot(xn[rows, :], wu[...], preferred_element_type=jnp.float32) * D ** (-0.5)
        hidden = jnp.maximum(hidden, 0.0)
        act[rows, :] = (hidden * hidden).astype(jnp.bfloat16)
        return carry

    lax.fori_loop(0, T // mrows, first, 0)

    scale = (F * 4) ** (-0.5)
    mine = pl.ds(pl.multiple_of(core * half, half), half)
    theirs = pl.ds(pl.multiple_of((1 - core) * half, half), half)
    turns = steps_of(line, per)
    total = line * 2 * per

    codes = []
    for n in range(total):
        (qa, sa, ha), (qb, sb, hb) = turns[0][0][n], turns[1][0][n]
        zz = jnp.where(inner, order_b[qb], order_b[qa])
        side = jnp.where(inner, jnp.int32(sb), jnp.int32(sa))
        h = jnp.where(inner, jnp.int32(hb), jnp.int32(ha))
        codes.append(((zz * 2 + x + side * (1 - 2 * x)) * per + h) * 2 + side)

    def code_of(n):
        got = jnp.int32(0)
        for i in range(total):
            got = got + jnp.where(n == i, codes[i], jnp.int32(0))
        return got

    def owner_of(b):
        o = b // nb
        return o, (o // 2) == chip

    def to_partner(b):
        return pltpu.make_async_remote_copy(
            src_ref=part.at[b], dst_ref=rin_p.at[b % nb], send_sem=a_send.at[b],
            recv_sem=a_recv.at[b % nb], device_id=(fs, partner), device_id_type=MESH)

    def swap(b):
        return pltpu.make_async_remote_copy(
            src_ref=part.at[b, theirs, :], dst_ref=pbuf.at[b], send_sem=b_send.at[b],
            recv_sem=b_recv.at[b], device_id=(fs, partner), device_id_type=MESH)

    def to_owner(b, o):
        return pltpu.make_async_remote_copy(
            src_ref=psum.at[b], dst_ref=rin_y.at[b % nb, mine, :], send_sem=c_send.at[b],
            recv_sem=c_recv.at[b % nb, core], device_id=(fs, o), device_id_type=MESH)

    def second_half(b):
        o, here = owner_of(b)

        @pl.when(jnp.logical_not(here))
        def _():
            swap(b).wait_recv()
            psum[b] = (part[b, mine, :].astype(jnp.float32)
                       + pbuf[b].astype(jnp.float32)).astype(jnp.bfloat16)
            to_owner(b, o).start()

    groups = {"early": early, "late": late}

    def event(q, what):
        if what == "two":
            relay(1, order_b[q], start, True, (), two)
        else:
            relay(1, order_b[q], start, True, groups[what], ())

    def body(n, carry):
        for role in range(2):
            mine_too = inner if role else outer
            for at, todo in turns[role][1].items():
                @pl.when((n == at) & mine_too)
                def _():
                    for q, what in todo:
                        event(q, what)
                    if role and at == turns[1][2]:
                        own_z(1, start, own_late & jnp.logical_not(low), own_late & low)

        code = code_of(n)
        b, side = code // 2, code % 2
        s, h = b // per, b % per
        for p in one:
            @pl.when((side == 1) & (h == pieces[p][0] // LANES))
            def _():
                piece(1, s, p, 2).wait_recv()
        rhs = wd[pl.ds(pl.multiple_of(b * LANES, LANES), LANES), :]
        product = lax.dot_general(act[...], rhs, (((1,), (1,)), ((), ())),
                                  preferred_element_type=jnp.float32)
        part[b] = (product * scale).astype(jnp.bfloat16)
        o, here = owner_of(b)

        @pl.when(here & (o != tp))
        def _():
            to_partner(b).start()

        @pl.when(jnp.logical_not(here))
        def _():
            swap(b).start()

        @pl.when(n > 0)
        def _():
            second_half(code_of(n - 1) // 2)

        return carry

    lax.fori_loop(0, total, body, 0)
    second_half(codes[total - 1] // 2)

    runs = nb // per if nb % per == 0 else 1
    for q in range(nb):
        i = (q % runs + x) % runs * (nb // runs) + q // runs
        b = tp * nb + i
        to_partner(b).wait_recv()
        for c in range(2):
            pltpu.make_async_remote_copy(
                src_ref=psum.at[b], dst_ref=rin_y.at[i, c * half:(c + 1) * half, :],
                send_sem=c_send.at[b], recv_sem=c_recv.at[i, c],
                device_id=(fs, partner), device_id_type=MESH).wait_recv()
        mixed[:, pl.ds(pl.multiple_of(i * LANES, LANES), LANES)] = (
            part[b].astype(jnp.float32) + rin_p[i].astype(jnp.float32)
            + rin_y[i].astype(jnp.float32)).astype(jnp.bfloat16)

    for slot, (k, to) in enumerate(((tp, mirror), (tp, partner), (mirror, partner))):
        tok_copy(xt.at[k], k, slot, to).wait_send()
    for a in range(2):
        own_x(a, wait_send, one + two)
        own_z(a, wait_send, has_up, has_dn)
        cross(a, wait_send, False)

    def drain(zz, carry):
        @pl.when(zz != z)
        def _():
            for a in range(2):
                relay(a, zz, wait_send, False, one, two)
        return carry

    lax.fori_loop(0, line, drain, 0)

    def drain_sums(b, carry):
        o, here = owner_of(b)

        @pl.when(here & (o != tp))
        def _():
            to_partner(b).wait_send()

        @pl.when(jnp.logical_not(here))
        def _():
            swap(b).wait_send()
            to_owner(b, o).wait_send()

        return carry

    lax.fori_loop(0, D // LANES, drain_sums, 0)


def steps_of(line, per):
    last = line - 1
    blocks, before = [], {}

    def add(q, side, hs):
        blocks.extend((q, side, h) for h in hs)

    def pass_on(*what):
        before.setdefault(len(blocks), []).extend(what)

    every, head, tail = range(per), range(per - 1), range(per - 1, per)
    add(0, 0, every)
    add(0, 1, every)
    add(1, 0, every)
    for q in range(2, line):
        pass_on((q, "early"))
        add(q - 1, 1, every)
        if q < last:
            pass_on((q, "late"), (q, "two"))
            add(q, 0, every)
    add(last, 0, head)
    pass_on((last, "late"))
    add(last, 1, head)
    pass_on((last, "two"))
    add(last, 0, tail)
    add(last, 1, tail)
    end = (blocks, before, max(before))

    blocks, before = [], {}
    add(0, 0, every)
    add(1, 0, every)
    for q in range(2, line):
        pass_on((q, "early"), (q, "late"), (q, "two"))
        add(q, 0, every)
    for q in range(line):
        add(q, 1, every)
    return end, (blocks, before, max(before))


def cut(r):
    across = min(LANES - 16, max(16, r * 5 // 32 // 8 * 8))
    got = []
    for first in range(0, r, LANES):
        rows = LANES if first + LANES < r else LANES - across
        lead = rows // 2 if rows == LANES else rows * 5 // 8 // 8 * 8
        got += [(first, lead, 1), (first + lead, rows - lead, 1)] if lead else [(first, rows, 1)]
    return got + [(r - across, across, 2)]


def fused(n_fs, prompt_tokens, norm_gain, up_master, down_master):
    T, dl = prompt_tokens.shape
    r, F = up_master.shape
    D = r * n_fs
    line = n_fs // 2
    pieces = cut(r)
    nblk, nb, half = D // LANES, dl // LANES, T // 2
    bf = jnp.bfloat16
    dma = pltpu.SemaphoreType.DMA
    vmem = pl.BlockSpec(memory_space=pltpu.VMEM)
    hbm = pl.BlockSpec(memory_space=pl.ANY)
    return pl.pallas_call(
        functools.partial(kernel, line, pieces),
        out_shape=(pltpu.VMEM((D, F), bf), pltpu.VMEM((D, F), bf), pltpu.VMEM((T, dl), bf)),
        in_specs=[hbm] * 4,
        out_specs=(vmem, vmem, vmem),
        scratch_shapes=[
            pltpu.VMEM((4, T, dl), bf), pltpu.VMEM((T, D), bf), pltpu.VMEM((T, F), bf),
            pltpu.VMEM((nblk, T, LANES), bf), pltpu.VMEM((nblk, half, LANES), bf),
            pltpu.VMEM((nblk, half, LANES), bf),
            pltpu.VMEM((nb, T, LANES), bf), pltpu.VMEM((nb, T, LANES), bf),
            dma((3, 2, n_fs, len(pieces))), dma((2, n_fs, len(pieces))),
            dma((3,)), dma((4,)),
            dma((nblk,)), dma((nb,)), dma((nblk,)), dma((nblk,)), dma((nblk,)), dma((nb, 2)),
            dma, pltpu.VMEM((r, F), jnp.float32), pltpu.VMEM((r, F), jnp.float32),
            pltpu.VMEM((1, r), jnp.float32), dma((3,)),
        ],
        compiler_params=pltpu.CompilerParams(
            collective_id=0, has_side_effects=True, vmem_limit_bytes=55 * 2 ** 20),
    )(prompt_tokens, norm_gain.reshape(1, r), up_master, down_master)


def put(src_a, src_b, src_c, dst_a, dst_b, dst_c, sem):
    copies = []
    for src, dst in ((src_a, dst_a), (src_b, dst_b), (src_c, dst_c)):
        n = 4 if src is not src_c else 1
        rows = src.shape[0] // n
        for i in range(n):
            part = pl.ds(i * rows, rows)
            copies.append(pltpu.make_async_copy(
                src.at[part, :], dst.at[part, :], sem.at[len(copies)]))
    for c in copies:
        c.start()
    for c in copies:
        c.wait()


def written(*arrays):
    hbm = pl.BlockSpec(memory_space=pl.ANY)
    return pl.pallas_call(
        put,
        out_shape=tuple(pltpu.HBM(a.shape, a.dtype) for a in arrays),
        in_specs=[pl.BlockSpec(memory_space=pltpu.VMEM)] * 3,
        out_specs=(pl.BlockSpec(memory_space=pltpu.HBM),) * 3,
        scratch_shapes=[pltpu.SemaphoreType.DMA((9,))],
        compiler_params=pltpu.CompilerParams(vmem_limit_bytes=2 ** 20),
    )(*(pltpu.with_memory_space_constraint(a, pltpu.VMEM) for a in arrays))


def solution(mesh):
    n_fs, n_tp = mesh.shape["fs"], mesh.shape["tp"]

    def shards(prompt_tokens, norm_gain, up_master, down_master):
        T, dl = prompt_tokens.shape
        r = up_master.shape[0]
        fits = (n_tp == 4 and n_fs % 2 == 0 and n_fs >= 6 and r % LANES == 0
                and dl % LANES == 0 and T % (2 * LANES) == 0 and r * n_fs == dl * n_tp)
        if not fits:
            return plain(prompt_tokens, norm_gain, up_master, down_master)
        return written(*fused(n_fs, prompt_tokens, norm_gain, up_master, down_master))

    return jax.shard_map(
        shards,
        mesh=mesh,
        in_specs=(P("fs", "tp"), P("fs"), P("fs", "tp"), P("fs", "tp")),
        out_specs=(P(None, "tp"), P(None, "tp"), P("fs", "tp")),
        check_vma=False,
    )
```

```python
import functools

import jax
import jax.numpy as jnp
from jax import lax
from jax.experimental import pallas as pl
from jax.experimental.pallas import tpu as pltpu
from jax.sharding import PartitionSpec as P

MESH = pl.DeviceIdType.MESH
LANES = 128


def plain(prompt_tokens, norm_gain, up_master, down_master):
    up_folded = (norm_gain[:, None] * up_master).astype(jnp.bfloat16)
    down_cast = down_master.astype(jnp.bfloat16)
    whole = lax.all_gather(prompt_tokens, "tp", axis=1, tiled=True)
    width = whole.shape[1]
    hidden_units = up_master.shape[1] * lax.axis_size("tp")
    wide = whole.astype(jnp.float32)
    normed = (wide * lax.rsqrt(jnp.mean(wide * wide, axis=1, keepdims=True) + 1e-05)).astype(
        jnp.bfloat16
    )
    contract = (((1,), (1,)), ((), ()))
    serve_up, serve_down = (
        lax.all_gather(up_folded, "fs", axis=0, tiled=True),
        lax.all_gather(down_cast, "fs", axis=0, tiled=True),
    )
    hidden = jnp.dot(normed, serve_up, preferred_element_type=jnp.float32)
    act = jnp.square(jax.nn.relu(hidden * width ** (-0.5))).astype(jnp.bfloat16)
    product = lax.dot_general(act, serve_down, contract, preferred_element_type=jnp.float32)
    partial_value = (product * hidden_units ** (-0.5)).astype(jnp.bfloat16)
    mixed = lax.psum_scatter(partial_value, "tp", scatter_dimension=1, tiled=True)
    return (serve_up, serve_down, mixed)


def kernel(line, pieces, tok, gain_hbm, up_hbm, down_hbm, wu, wd, mixed,
           xt, xn, act, part, pbuf, psum, rin_p, rin_y,
           w_send, z_recv, x_recv, xa_recv, xb_recv, t_send, t_recv,
           a_send, a_recv, b_send, b_recv, c_send, c_recv,
           l_sem, up, down, gain, d_sem):
    T, dl = tok.shape
    r, F = up_hbm.shape
    D = wu.shape[0]
    tp = lax.axis_index("tp")
    fs = lax.axis_index("fs")
    z, x = fs // 2, fs % 2
    core, chip = tp % 2, tp // 2
    partner = tp + 1 - 2 * core
    mirror = (tp + 2) % 4
    diag = (partner + 2) % 4
    has_up, has_dn = z < line - 1, z > 0
    inner = has_up & has_dn
    outer = jnp.logical_not(inner)
    low = z < line / 2
    high = jnp.logical_not(low)
    W = (wu, wd)
    nb = dl // LANES
    per = r // LANES
    half = T // 2
    zdev = ((fs + 2, tp), (fs - 2, tp), (fs + 1 - 2 * x, tp))

    barrier = pltpu.get_barrier_semaphore()

    def greet(dev):
        pl.semaphore_signal(barrier, inc=1, device_id=dev, device_id_type=MESH)

    greet(zdev[2])
    pl.when(has_up)(lambda: greet(zdev[0]))
    pl.when(has_dn)(lambda: greet(zdev[1]))
    for other in (mirror, diag, partner):
        greet((fs, other))

    def lane_rows(i):
        return slice(i * LANES, (i + 1) * LANES)

    load_gain = pltpu.make_async_copy(gain_hbm, gain, d_sem.at[per])
    load_up = [pltpu.make_async_copy(up_hbm.at[lane_rows(i), :], up.at[lane_rows(i), :],
                                     d_sem.at[i]) for i in range(per)]
    load_down = pltpu.make_async_copy(down_hbm, down, d_sem.at[per + 1])
    own_tok = pltpu.make_async_copy(tok, xt.at[tp], l_sem)
    for load in [load_gain] + load_up + [own_tok, load_down]:
        load.start()

    base = pl.multiple_of(fs * r, r)

    def fold(i):
        load_up[i].wait()
        rows = lane_rows(i)
        g = jnp.transpose(jnp.broadcast_to(gain[:, rows], (LANES, LANES)))
        for c in range(F // LANES):
            cols = lane_rows(c)
            wu[pl.ds(base + i * LANES, LANES), cols] = (g * up[rows, cols]).astype(jnp.bfloat16)

    one = [p for p in range(len(pieces)) if pieces[p][2] == 1]
    two = [p for p in range(len(pieces)) if pieces[p][2] == 2][0]
    across = pieces[two][1]
    single = r - across

    def block_at(p):
        return pieces[p][0] // LANES

    def rows_of(a, first, size):
        return W[a].at[pl.ds(pl.multiple_of(first, 8), size), :]

    def remote(ref, send_sem, recv_sem, way):
        return pltpu.make_async_remote_copy(
            src_ref=ref, dst_ref=ref, send_sem=send_sem, recv_sem=recv_sem,
            device_id=zdev[way], device_id_type=MESH)

    def piece(a, s, p, way):
        if way < 2:
            recv = z_recv.at[a, s // 2, p]
        elif p == two:
            recv = x_recv.at[a]
        else:
            recv = xb_recv.at[s // 2, block_at(p)] if a else xa_recv
        return remote(rows_of(a, s * r + pieces[p][0], pieces[p][1]), w_send.at[way, a], recv, way)

    def tok_copy(src, k, to):
        return pltpu.make_async_remote_copy(
            src_ref=src, dst_ref=xt.at[k], send_sem=t_send, recv_sem=t_recv.at[k],
            device_id=(fs, to), device_id_type=MESH)

    def send_z(a, s, which, up_cond, dn_cond):
        for p in which:
            pl.when(up_cond)(lambda: piece(a, s, p, 0).start())
            pl.when(dn_cond)(lambda: piece(a, s, p, 1).start())

    def send_x(a, s, which):
        for p in which:
            piece(a, s, p, 2).start()

    xs = fs + 1 - 2 * x

    def near(i, k):
        return (abs(k - i), -k if i < line / 2 else k)

    def chip_of(k):
        return (2 * k * per // nb) // 2

    def pick(table):
        got = jnp.int32(0)
        for i in range(line):
            for y in range(2):
                got = got + jnp.where((z == i) & (chip == y), jnp.int32(table(i, y)), jnp.int32(0))
        return got

    order_a = [pick(lambda i, y: sorted(range(line), key=lambda k: near(i, k))[q])
               for q in range(line)]
    order_b = [pick(lambda i, y: sorted(range(line), key=lambda k: (
        k != i, chip_of(k) == y, near(i, k)))[q]) for q in range(line)]
    own_late = inner & (pick(lambda i, y: int(chip_of(i) == y)) == 1)

    def pass_one(a, zz, p):
        same = zz * 2 + x
        piece(a, same, p, 0).wait_recv()
        send_z(a, same, [p], (zz < z) & has_up, (zz > z) & has_dn)
        send_x(a, same, [p])

    def pass_two(a, zz):
        remote(rows_of(a, zz * 2 * r, 2 * across), w_send.at[0, a], z_recv.at[a, zz, two], 0).wait_recv()
        for s in (zz * 2 + x, zz * 2 + 1 - x):
            send_z(a, s, [two], (zz < z) & has_up, (zz > z) & has_dn)

    def send_two(a, up_cond, dn_cond):
        for s in (fs, xs):
            send_z(a, s, [two], up_cond, dn_cond)

    def forward_tokens():
        tok_copy(xt.at[mirror], mirror, mirror).wait_recv()
        tok_copy(xt.at[mirror], mirror, partner).start()

    load_gain.wait()
    for i in range(per):
        fold(i)
    links = 4 + has_up.astype(jnp.int32) + has_dn.astype(jnp.int32)
    pl.semaphore_wait(barrier, links)
    send_x(0, fs, [two])
    send_z(0, fs, one + [two], has_up, has_dn)
    send_x(0, fs, one)
    own_tok.wait()
    tok_copy(xt.at[tp], tp, mirror).start()
    tok_copy(xt.at[tp], tp, partner).start()
    load_down.wait()
    wd[pl.ds(base, r), :] = down[...].astype(jnp.bfloat16)
    pl.when(inner)(lambda: send_x(1, fs, [two]))
    piece(0, xs, two, 2).wait_recv()
    send_z(0, xs, [two], has_up, has_dn)
    send_z(1, fs, one + [two], outer & has_up, outer & has_dn)
    ahead = jnp.logical_not(own_late)

    for idx in range(1, line):
        for p in one:
            pass_one(0, order_a[idx], p)
        if idx == line - 2:
            @pl.when(outer)
            def _():
                send_x(1, fs, [two])
                forward_tokens()
        if idx == line - 1:
            @pl.when(outer)
            def _():
                send_x(1, fs, FILL[0])

            @pl.when(inner)
            def _():
                send_x(1, fs, one)
                forward_tokens()
        pass_two(0, order_a[idx])
        if idx == line - 2:
            @pl.when(inner)
            def _():
                send_z(1, fs, one, low, high)
                piece(1, xs, two, 2).wait_recv()
                send_two(1, low, high)

    @pl.when(inner)
    def _():
        send_z(1, fs, one, ahead & high, ahead & low)

    @pl.when(outer)
    def _():
        piece(1, xs, two, 2).wait_recv()
        send_z(1, xs, [two], has_up, has_dn)

    tok_copy(xt.at[partner], partner, partner).wait_recv()
    tok_copy(xt.at[diag], diag, partner).wait_recv()
    block = 64

    def norm(i, carry):
        rows = pl.ds(pl.multiple_of(i * block, block), block)
        wide = [xt[k, rows, :].astype(jnp.float32) for k in range(4)]
        sq = wide[0] * wide[0]
        for k in range(1, 4):
            sq = sq + wide[k] * wide[k]
        inv = lax.rsqrt(jnp.sum(sq, axis=1, keepdims=True) * (1.0 / D) + 1e-05)
        for k in range(4):
            xn[rows, k * dl:(k + 1) * dl] = (wide[k] * inv).astype(jnp.bfloat16)
        return carry

    lax.fori_loop(0, T // block, norm, 0)

    for p in one:
        pass_one(1, order_b[1], p)

    @pl.when(outer)
    def _():
        send_x(1, fs, FILL[1])

    @pl.when(inner)
    def _():
        for p in EARLY:
            pass_one(1, order_b[2], p)

    remote(rows_of(0, 0, line * single), w_send.at[2, 0], xa_recv, 2).wait_recv()

    mrows = 2 * LANES

    def first(i, carry):
        rows = pl.ds(pl.multiple_of(i * mrows, mrows), mrows)
        hidden = jnp.dot(xn[rows, :], wu[...], preferred_element_type=jnp.float32) * D ** (-0.5)
        hidden = jnp.maximum(hidden, 0.0)
        act[rows, :] = (hidden * hidden).astype(jnp.bfloat16)
        return carry

    lax.fori_loop(0, T // mrows, first, 0)

    scale = (F * 4) ** (-0.5)
    mine = pl.ds(pl.multiple_of(core * half, half), half)
    theirs = pl.ds(pl.multiple_of((1 - core) * half, half), half)
    total = line * 2 * per

    codes = []
    for n in range(total):
        (qa, sa, ha), (qb, sb, hb) = END[n][0], INNER[n][0]
        zz = jnp.where(inner, order_b[qb], order_b[qa])
        side = jnp.where(inner, jnp.int32(sb), jnp.int32(sa))
        h = jnp.where(inner, jnp.int32(hb), jnp.int32(ha))
        codes.append(((zz * 2 + x + side * (1 - 2 * x)) * per + h) * 2 + side)

    def code_of(n):
        got = jnp.int32(0)
        for i in range(total):
            got = got + jnp.where(n == i, codes[i], jnp.int32(0))
        return got

    def owner_of(b):
        o = b // nb
        return o, (o // 2) == chip

    away = 2 * nb

    def to_partner(b):
        return pltpu.make_async_remote_copy(
            src_ref=part.at[b], dst_ref=rin_p.at[b % nb], send_sem=a_send,
            recv_sem=a_recv.at[b % nb], device_id=(fs, partner), device_id_type=MESH)

    def swap(b):
        return pltpu.make_async_remote_copy(
            src_ref=part.at[b, theirs, :], dst_ref=pbuf.at[b % away], send_sem=b_send,
            recv_sem=b_recv.at[b % away], device_id=(fs, partner), device_id_type=MESH)

    def to_owner(b, o):
        return pltpu.make_async_remote_copy(
            src_ref=psum.at[b % away], dst_ref=rin_y.at[b % nb, mine, :], send_sem=c_send,
            recv_sem=c_recv.at[b % nb], device_id=(fs, o), device_id_type=MESH)

    def second_half(b):
        o, here = owner_of(b)

        @pl.when(jnp.logical_not(here))
        def _():
            swap(b).wait_recv()
            psum[b % away] = (part[b, mine, :].astype(jnp.float32)
                              + pbuf[b % away].astype(jnp.float32)).astype(jnp.bfloat16)
            to_owner(b, o).start()

    def event(q, what):
        if what == "two":
            pass_two(1, order_b[q])
        elif what == "fill":
            send_x(1, fs, FILL[2])
        elif what == "own":
            send_z(1, fs, one, own_late & high, own_late & low)
            send_two(1, own_late & high, own_late & low)
        elif what == "own two":
            send_two(1, ahead & high, ahead & low)
        else:
            pass_one(1, order_b[q], what)

    def body(n, carry):
        for here, table in ((outer, END), (inner, INNER)):
            @pl.when(here)
            def _():
                for at in range(total):
                    if table[at][1]:
                        @pl.when(n == at)
                        def _():
                            for q, what in table[at][1]:
                                event(q, what)

        code = code_of(n)
        b, side = code // 2, code % 2
        s, h = b // per, b % per

        @pl.when(side == 1)
        def _():
            for i in range(per):
                size = sum(pieces[p][1] for p in one if block_at(p) == i)
                pl.when(h == i)(lambda: remote(
                    rows_of(1, s * r + i * LANES, size), w_send.at[2, 1],
                    xb_recv.at[s // 2, i], 2).wait_recv())

        rhs = wd[pl.ds(pl.multiple_of(b * LANES, LANES), LANES), :]
        product = lax.dot_general(act[...], rhs, (((1,), (1,)), ((), ())),
                                  preferred_element_type=jnp.float32)
        part[b] = (product * scale).astype(jnp.bfloat16)
        o, here = owner_of(b)

        @pl.when(here & (o != tp))
        def _():
            to_partner(b).start()

        @pl.when(jnp.logical_not(here))
        def _():
            swap(b).start()

        @pl.when(n > 0)
        def _():
            second_half(code_of(n - 1) // 2)

        return carry

    lax.fori_loop(0, total, body, 0)
    second_half(codes[total - 1] // 2)

    runs = nb // per if nb % per == 0 else 1
    for q in range(nb):
        i = (q % runs + x) % runs * (nb // runs) + q // runs
        b = tp * nb + i
        to_partner(b).wait_recv()
        pltpu.make_async_remote_copy(
            src_ref=part.at[b], dst_ref=rin_y.at[i], send_sem=c_send, recv_sem=c_recv.at[i],
            device_id=(fs, partner), device_id_type=MESH).wait_recv()
        mixed[:, pl.ds(pl.multiple_of(i * LANES, LANES), LANES)] = (
            part[b].astype(jnp.float32) + rin_p[i].astype(jnp.float32)
            + rin_y[i].astype(jnp.float32)).astype(jnp.bfloat16)

    def drain(ref, sem):
        pltpu.make_async_remote_copy(
            src_ref=ref, dst_ref=ref, send_sem=sem, recv_sem=l_sem,
            device_id=(fs, partner), device_id_type=MESH).wait_send()

    drain(xt.at[0:3], t_send)
    for a in range(2):
        drain(rows_of(a, 0, r + (line - 1) * single), w_send.at[2, a])
        for i in range(line):
            @pl.when(z == i)
            def _():
                if i < line - 1:
                    drain(rows_of(a, 0, (i + 1) * (r + across)), w_send.at[0, a])
                if i > 0:
                    drain(rows_of(a, 0, (line - i) * (r + across)), w_send.at[1, a])
    drain(part.at[0:nb], a_send)
    drain(pbuf, b_send)
    drain(psum, c_send)


END = (
    ((0, 0, 0), ((2, 0),)), ((0, 0, 1), ()),
    ((1, 0, 0), ((2, 1),)), ((1, 1, 0), ()),
    ((2, 0, 0), ((2, 2), (2, 3), (0, "fill"))),
    ((1, 0, 1), ((1, "two"),)), ((1, 1, 1), ()), ((2, 1, 0), ()),
    ((2, 0, 1), ((2, "two"),)), ((2, 1, 1), ()),
    ((0, 1, 0), ((3, 0),)), ((3, 0, 0), ((3, 1),)), ((0, 1, 1), ()),
    ((3, 1, 0), ((3, 2), (3, 3))), ((3, 0, 1), ((3, "two"),)), ((3, 1, 1), ()),
)
INNER = (
    ((0, 0, 0), ((2, 2), (2, 3), (1, "two"), (0, "own two"))), ((0, 0, 1), ()),
    ((1, 0, 0), ()), ((1, 0, 1), ()),
    ((2, 0, 0), ((2, "two"),)), ((2, 0, 1), ()),
    ((0, 1, 0), ()), ((0, 1, 1), ()),
    ((1, 1, 0), ((3, 0), (3, 1))), ((1, 1, 1), ()),
    ((3, 0, 0), ((3, 2), (3, 3), (3, "two"), (0, "own"))), ((3, 0, 1), ()),
    ((2, 1, 0), ()), ((2, 1, 1), ()), ((3, 1, 0), ()), ((3, 1, 1), ()),
)
EARLY = (0, 1)
FILL = ((0,), (3,), (1, 2))


def cut(r):
    across = r * 5 // 32 // 8 * 8
    lead = (LANES - across) * 5 // 8 // 8 * 8
    h = LANES // 2
    return [(0, h, 1), (h, h, 1), (LANES, lead, 1),
            (LANES + lead, LANES - across - lead, 1), (r - across, across, 2)]


def fused(n_fs, prompt_tokens, norm_gain, up_master, down_master):
    T, dl = prompt_tokens.shape
    r, F = up_master.shape
    D = r * n_fs
    line = n_fs // 2
    pieces = cut(r)
    nblk, nb, half = D // LANES, dl // LANES, T // 2
    bf = jnp.bfloat16
    dma = pltpu.SemaphoreType.DMA
    vmem = pl.BlockSpec(memory_space=pltpu.VMEM)
    hbm = pl.BlockSpec(memory_space=pl.ANY)
    return pl.pallas_call(
        functools.partial(kernel, line, pieces),
        out_shape=(pltpu.VMEM((D, F), bf), pltpu.VMEM((D, F), bf), pltpu.VMEM((T, dl), bf)),
        in_specs=[hbm] * 4,
        out_specs=(vmem, vmem, vmem),
        scratch_shapes=[
            pltpu.VMEM((4, T, dl), bf), pltpu.VMEM((T, D), bf), pltpu.VMEM((T, F), bf),
            pltpu.VMEM((nblk, T, LANES), bf), pltpu.VMEM((2 * nb, half, LANES), bf),
            pltpu.VMEM((2 * nb, half, LANES), bf),
            pltpu.VMEM((nb, T, LANES), bf), pltpu.VMEM((nb, T, LANES), bf),
            dma((3, 2)), dma((2, line, len(pieces))), dma((2,)), dma, dma((line, r // LANES)),
            dma, dma((4,)),
            dma, dma((nb,)), dma, dma((2 * nb,)), dma, dma((nb,)),
            dma, pltpu.VMEM((r, F), jnp.float32), pltpu.VMEM((r, F), jnp.float32),
            pltpu.VMEM((1, r), jnp.float32), dma((r // LANES + 2,)),
        ],
        compiler_params=pltpu.CompilerParams(
            collective_id=0, has_side_effects=True, vmem_limit_bytes=55 * 2 ** 20),
    )(prompt_tokens, norm_gain.reshape(1, r), up_master, down_master)


def put(src_a, src_b, src_c, dst_a, dst_b, dst_c, sem):
    copies = []
    for src, dst in ((src_a, dst_a), (src_b, dst_b), (src_c, dst_c)):
        n = 4 if src is not src_c else 1
        rows = src.shape[0] // n
        for i in range(n):
            part = pl.ds(i * rows, rows)
            copies.append(pltpu.make_async_copy(
                src.at[part, :], dst.at[part, :], sem.at[len(copies)]))
    for c in copies:
        c.start()
    for c in copies:
        c.wait()


def written(*arrays):
    hbm = pl.BlockSpec(memory_space=pl.ANY)
    return pl.pallas_call(
        put,
        out_shape=tuple(pltpu.HBM(a.shape, a.dtype) for a in arrays),
        in_specs=[pl.BlockSpec(memory_space=pltpu.VMEM)] * 3,
        out_specs=(pl.BlockSpec(memory_space=pltpu.HBM),) * 3,
        scratch_shapes=[pltpu.SemaphoreType.DMA((9,))],
        compiler_params=pltpu.CompilerParams(vmem_limit_bytes=2 ** 20),
    )(*(pltpu.with_memory_space_constraint(a, pltpu.VMEM) for a in arrays))


def solution(mesh):
    n_fs, n_tp = mesh.shape["fs"], mesh.shape["tp"]

    def shards(prompt_tokens, norm_gain, up_master, down_master):
        T, dl = prompt_tokens.shape
        r = up_master.shape[0]
        fits = (n_tp == 4 and n_fs == 8 and r == 2 * LANES
                and dl % LANES == 0 and T % (2 * LANES) == 0 and r * n_fs == dl * n_tp)
        if not fits:
            return plain(prompt_tokens, norm_gain, up_master, down_master)
        return written(*fused(n_fs, prompt_tokens, norm_gain, up_master, down_master))

    return jax.shard_map(
        shards,
        mesh=mesh,
        in_specs=(P("fs", "tp"), P("fs"), P("fs", "tp"), P("fs", "tp")),
        out_specs=(P(None, "tp"), P(None, "tp"), P("fs", "tp")),
        check_vma=False,
    )
```

```python
import functools

import jax
import jax.numpy as jnp
from jax import lax
from jax.experimental import pallas as pl
from jax.experimental.pallas import tpu as pltpu
from jax.sharding import PartitionSpec as P

MESH = pl.DeviceIdType.MESH
LANES = 128


def plain(prompt_tokens, norm_gain, up_master, down_master):
    up_folded = (norm_gain[:, None] * up_master).astype(jnp.bfloat16)
    down_cast = down_master.astype(jnp.bfloat16)
    whole = lax.all_gather(prompt_tokens, "tp", axis=1, tiled=True)
    width = whole.shape[1]
    hidden_units = up_master.shape[1] * lax.axis_size("tp")
    wide = whole.astype(jnp.float32)
    normed = (wide * lax.rsqrt(jnp.mean(wide * wide, axis=1, keepdims=True) + 1e-05)).astype(
        jnp.bfloat16
    )
    contract = (((1,), (1,)), ((), ()))
    serve_up, serve_down = (
        lax.all_gather(up_folded, "fs", axis=0, tiled=True),
        lax.all_gather(down_cast, "fs", axis=0, tiled=True),
    )
    hidden = jnp.dot(normed, serve_up, preferred_element_type=jnp.float32)
    act = jnp.square(jax.nn.relu(hidden * width ** (-0.5))).astype(jnp.bfloat16)
    product = lax.dot_general(act, serve_down, contract, preferred_element_type=jnp.float32)
    partial_value = (product * hidden_units ** (-0.5)).astype(jnp.bfloat16)
    mixed = lax.psum_scatter(partial_value, "tp", scatter_dimension=1, tiled=True)
    return (serve_up, serve_down, mixed)


def kernel(line, pieces, tok, gain_hbm, up_hbm, down_hbm, wu, wd, mixed,
           xt, xn, act, part, pbuf, psum, rin_p, rin_y,
           w_send, z_recv, x_recv, xa_recv, xb_recv, t_send, t_recv,
           a_send, a_recv, b_send, b_recv, c_send, c_recv,
           l_sem, up, down, gain, d_sem):
    T, dl = tok.shape
    r, F = up_hbm.shape
    D = wu.shape[0]
    tp = lax.axis_index("tp")
    fs = lax.axis_index("fs")
    z, x = fs // 2, fs % 2
    core, chip = tp % 2, tp // 2
    partner = tp + 1 - 2 * core
    mirror = (tp + 2) % 4
    diag = (partner + 2) % 4
    has_up, has_dn = z < line - 1, z > 0
    inner = has_up & has_dn
    outer = jnp.logical_not(inner)
    low = z < line / 2
    high = jnp.logical_not(low)
    W = (wu, wd)
    nb = dl // LANES
    per = r // LANES
    half = T // 2
    zdev = ((fs + 2, tp), (fs - 2, tp), (fs + 1 - 2 * x, tp))

    barrier = pltpu.get_barrier_semaphore()

    def greet(dev):
        pl.semaphore_signal(barrier, inc=1, device_id=dev, device_id_type=MESH)

    greet(zdev[2])
    pl.when(has_up)(lambda: greet(zdev[0]))
    pl.when(has_dn)(lambda: greet(zdev[1]))
    for other in (mirror, diag, partner):
        greet((fs, other))

    parts = len(pieces[0])
    one, two = list(range(parts - 1)), parts - 1

    def lane_rows(i):
        return slice(i * LANES, (i + 1) * LANES)

    load_gain = pltpu.make_async_copy(gain_hbm, gain, d_sem.at[parts])
    def piece_rows(p):
        return slice(pieces[0][p][0], sum(pieces[0][p]))

    load_up = [pltpu.make_async_copy(up_hbm.at[piece_rows(p), :], up.at[piece_rows(p), :],
                                     d_sem.at[p]) for p in range(parts)]
    load_down = pltpu.make_async_copy(down_hbm, down, d_sem.at[parts + 1])
    own_tok = pltpu.make_async_copy(tok, xt.at[tp], l_sem)
    for load in [load_gain] + [load_up[p] for p in [two] + one] + [own_tok, load_down]:
        load.start()

    base = pl.multiple_of(fs * r, r)

    def gains(i):
        return jnp.transpose(jnp.broadcast_to(gain[:, lane_rows(i)], (LANES, LANES)))

    def fold(p):
        load_up[p].wait()
        at, size = pieces[0][p]
        g = column[at // LANES][at % LANES:at % LANES + size]
        for c in range(F // LANES):
            cols = lane_rows(c)
            wu[pl.ds(pl.multiple_of(base + at, 8), size), cols] = (
                g * up[at:at + size, cols]).astype(jnp.bfloat16)

    across = [pieces[a][two][1] for a in range(2)]

    def block_at(p):
        return pieces[1][p][0] // LANES

    def rows_of(a, first, size):
        return W[a].at[pl.ds(pl.multiple_of(first, 8), size), :]

    def remote(ref, send_sem, recv_sem, way):
        return pltpu.make_async_remote_copy(
            src_ref=ref, dst_ref=ref, send_sem=send_sem, recv_sem=recv_sem,
            device_id=zdev[way], device_id_type=MESH)

    def piece(a, s, p, way):
        if way < 2:
            recv = z_recv.at[a, (s // 2 - z + (2, 0)[way]) % line, p]
        elif p == two:
            recv = x_recv.at[a]
        else:
            recv = xb_recv.at[s // 2, block_at(p)] if a else xa_recv
        return remote(rows_of(a, s * r + pieces[a][p][0], pieces[a][p][1]), w_send.at[way, a], recv, way)

    def tok_copy(src, k, to):
        return pltpu.make_async_remote_copy(
            src_ref=src, dst_ref=xt.at[k], send_sem=t_send, recv_sem=t_recv.at[k],
            device_id=(fs, to), device_id_type=MESH)

    def send_z(a, s, which, up_cond, dn_cond):
        for p in which:
            pl.when(up_cond)(lambda: piece(a, s, p, 0).start())
            pl.when(dn_cond)(lambda: piece(a, s, p, 1).start())

    def send_x(a, s, which):
        for p in which:
            piece(a, s, p, 2).start()

    xs = fs + 1 - 2 * x

    def near(i, k):
        return (abs(k - i), -k if i < line / 2 else k)

    def chip_of(k):
        return (2 * k * per // nb) // 2

    def pick(table):
        got = jnp.int32(0)
        for i in range(line):
            for y in range(2):
                got = got + jnp.where((z == i) & (chip == y), jnp.int32(table(i, y)), jnp.int32(0))
        return got

    order_a = [pick(lambda i, y: sorted(range(line), key=lambda k: near(i, k))[q])
               for q in range(line)]
    order_b = [pick(lambda i, y: sorted(range(line), key=lambda k: (
        k != i, chip_of(k) == y, near(i, k)))[q]) for q in range(line)]
    own_late = inner & (pick(lambda i, y: int(chip_of(i) == y)) == 1)

    def arrived(a, zz, p, first, size):
        remote(rows_of(a, first, size), w_send.at[0, a],
               z_recv.at[a, (zz - z + line - 1) % line, p], 0).wait_recv()

    def pass_one(a, zz, p):
        same = zz * 2 + x
        arrived(a, zz, p, same * r + pieces[a][p][0], pieces[a][p][1])
        send_z(a, same, [p], (zz < z) & has_up, (zz > z) & has_dn)
        send_x(a, same, [p])

    def pass_two(a, zz):
        arrived(a, zz, two, zz * 2 * r, 2 * across[a])
        for s in (zz * 2 + x, zz * 2 + 1 - x):
            send_z(a, s, [two], (zz < z) & has_up, (zz > z) & has_dn)

    def send_two(a, up_cond, dn_cond):
        for s in (fs, xs):
            send_z(a, s, [two], up_cond, dn_cond)

    def forward_tokens():
        tok_copy(xt.at[mirror], mirror, mirror).wait_recv()
        tok_copy(xt.at[mirror], mirror, partner).start()

    load_gain.wait()
    column = [gains(i) for i in range(per)]
    links = 4 + has_up.astype(jnp.int32) + has_dn.astype(jnp.int32)
    fold(two)
    fold(one[0])
    pl.semaphore_wait(barrier, links)
    send_x(0, fs, [two])
    for p in one:
        if p != one[0]:
            fold(p)
        send_z(0, fs, [p], has_up, has_dn)
        send_x(0, fs, [p])
    send_z(0, fs, [two], has_up, has_dn)
    own_tok.wait()
    tok_copy(xt.at[tp], tp, mirror).start()
    tok_copy(xt.at[tp], tp, partner).start()
    load_down.wait()
    wd[pl.ds(base, r), :] = down[...].astype(jnp.bfloat16)
    pl.when(inner)(lambda: send_x(1, fs, [two]))
    piece(0, xs, two, 2).wait_recv()
    send_z(0, xs, [two], has_up, has_dn)
    send_z(1, fs, one + [two], outer & has_up, outer & has_dn)
    ahead = jnp.logical_not(own_late)

    for idx in range(1, line):
        for p in one:
            pass_one(0, order_a[idx], p)
        if idx == line - 2:
            @pl.when(outer)
            def _():
                send_x(1, fs, [two])
                forward_tokens()
        if idx == line - 1:
            @pl.when(outer)
            def _():
                send_x(1, fs, FILL[0])

            @pl.when(inner)
            def _():
                send_x(1, fs, one)
                forward_tokens()
        pass_two(0, order_a[idx])
        if idx == line - 2:
            @pl.when(inner)
            def _():
                send_z(1, fs, one, low, high)
                piece(1, xs, two, 2).wait_recv()
                send_two(1, low, high)

    @pl.when(inner)
    def _():
        send_z(1, fs, one, ahead & high, ahead & low)

    @pl.when(outer)
    def _():
        piece(1, xs, two, 2).wait_recv()
        send_z(1, xs, [two], has_up, has_dn)

    tok_copy(xt.at[partner], partner, partner).wait_recv()
    tok_copy(xt.at[diag], diag, partner).wait_recv()
    block = 64

    def norm(i, carry):
        rows = pl.ds(pl.multiple_of(i * block, block), block)
        wide = [xt[k, rows, :].astype(jnp.float32) for k in range(4)]
        sq = wide[0] * wide[0]
        for k in range(1, 4):
            sq = sq + wide[k] * wide[k]
        inv = lax.rsqrt(jnp.sum(sq, axis=1, keepdims=True) * (1.0 / D) + 1e-05)
        for k in range(4):
            xn[rows, k * dl:(k + 1) * dl] = (wide[k] * inv).astype(jnp.bfloat16)
        return carry

    lax.fori_loop(0, T // block, norm, 0)

    for p in one:
        pass_one(1, order_b[1], p)

    @pl.when(outer)
    def _():
        send_x(1, fs, FILL[1])

    @pl.when(inner)
    def _():
        for p in EARLY:
            pass_one(1, order_b[2], p)

    remote(rows_of(0, 0, line * (r - across[0])), w_send.at[2, 0], xa_recv, 2).wait_recv()

    mrows = 2 * LANES

    def first(i, carry):
        rows = pl.ds(pl.multiple_of(i * mrows, mrows), mrows)
        hidden = jnp.dot(xn[rows, :], wu[...], preferred_element_type=jnp.float32) * D ** (-0.5)
        hidden = jnp.maximum(hidden, 0.0)
        act[rows, :] = (hidden * hidden).astype(jnp.bfloat16)
        for k, p in enumerate(BETWEEN):
            pl.when(inner & (i == min(k, T // mrows - 1)))(lambda: pass_one(1, order_b[2], p))
        return carry

    lax.fori_loop(0, T // mrows, first, 0)

    scale = (F * 4) ** (-0.5)
    mine = pl.ds(pl.multiple_of(core * half, half), half)
    theirs = pl.ds(pl.multiple_of((1 - core) * half, half), half)
    total = line * 2 * per

    codes = []
    for n in range(total):
        (qa, sa, ha), (qb, sb, hb) = END[n][0], INNER[n][0]
        zz = jnp.where(inner, order_b[qb], order_b[qa])
        side = jnp.where(inner, jnp.int32(sb), jnp.int32(sa))
        h = jnp.where(inner, jnp.int32(hb), jnp.int32(ha))
        codes.append(((zz * 2 + x + side * (1 - 2 * x)) * per + h) * 2 + side)

    def code_of(n):
        got = jnp.int32(0)
        for i in range(total):
            got = got + jnp.where(n == i, codes[i], jnp.int32(0))
        return got

    def owner_of(b):
        o = b // nb
        return o, (o // 2) == chip

    away = 2 * nb

    def to_partner(b):
        return pltpu.make_async_remote_copy(
            src_ref=part.at[b], dst_ref=rin_p.at[b % nb], send_sem=a_send,
            recv_sem=a_recv.at[b % nb], device_id=(fs, partner), device_id_type=MESH)

    def swap(b):
        return pltpu.make_async_remote_copy(
            src_ref=part.at[b, theirs, :], dst_ref=pbuf.at[b % away], send_sem=b_send,
            recv_sem=b_recv.at[b % away], device_id=(fs, partner), device_id_type=MESH)

    def to_owner(b, o):
        return pltpu.make_async_remote_copy(
            src_ref=psum.at[b % away], dst_ref=rin_y.at[b % nb, mine, :], send_sem=c_send,
            recv_sem=c_recv.at[b % nb], device_id=(fs, o), device_id_type=MESH)

    def second_half(b):
        o, here = owner_of(b)

        @pl.when(jnp.logical_not(here))
        def _():
            swap(b).wait_recv()
            psum[b % away] = (part[b, mine, :].astype(jnp.float32)
                              + pbuf[b % away].astype(jnp.float32)).astype(jnp.bfloat16)
            to_owner(b, o).start()

    def event(q, what):
        if what == "two":
            pass_two(1, order_b[q])
        elif what == "fill":
            send_x(1, fs, FILL[2])
        elif what == "own":
            send_z(1, fs, one, own_late & high, own_late & low)
            send_two(1, own_late & high, own_late & low)
        elif what == "own two":
            send_two(1, ahead & high, ahead & low)
        else:
            pass_one(1, order_b[q], what)

    def body(n, carry):
        for here, table in ((outer, END), (inner, INNER)):
            @pl.when(here)
            def _():
                for at in range(total):
                    if table[at][1]:
                        @pl.when(n == at)
                        def _():
                            for q, what in table[at][1]:
                                event(q, what)

        code = code_of(n)
        b, side = code // 2, code % 2
        s, h = b // per, b % per

        @pl.when(side == 1)
        def _():
            for i in range(per):
                size = sum(pieces[1][p][1] for p in one if block_at(p) == i)
                pl.when(h == i)(lambda: remote(
                    rows_of(1, s * r + i * LANES, size), w_send.at[2, 1],
                    xb_recv.at[s // 2, i], 2).wait_recv())

        rhs = wd[pl.ds(pl.multiple_of(b * LANES, LANES), LANES), :]
        product = lax.dot_general(act[...], rhs, (((1,), (1,)), ((), ())),
                                  preferred_element_type=jnp.float32)
        part[b] = (product * scale).astype(jnp.bfloat16)
        o, here = owner_of(b)

        @pl.when(here & (o != tp))
        def _():
            to_partner(b).start()

        @pl.when(jnp.logical_not(here))
        def _():
            swap(b).start()

        @pl.when(n > 0)
        def _():
            second_half(code_of(n - 1) // 2)

        return carry

    lax.fori_loop(0, total, body, 0)
    second_half(codes[total - 1] // 2)

    runs = nb // per if nb % per == 0 else 1
    for q in range(nb):
        i = (q % runs + x) % runs * (nb // runs) + q // runs
        b = tp * nb + i
        to_partner(b).wait_recv()
        pltpu.make_async_remote_copy(
            src_ref=part.at[b], dst_ref=rin_y.at[i], send_sem=c_send, recv_sem=c_recv.at[i],
            device_id=(fs, partner), device_id_type=MESH).wait_recv()
        mixed[:, pl.ds(pl.multiple_of(i * LANES, LANES), LANES)] = (
            part[b].astype(jnp.float32) + rin_p[i].astype(jnp.float32)
            + rin_y[i].astype(jnp.float32)).astype(jnp.bfloat16)

    def drain(ref, sem):
        pltpu.make_async_remote_copy(
            src_ref=ref, dst_ref=ref, send_sem=sem, recv_sem=l_sem,
            device_id=(fs, partner), device_id_type=MESH).wait_send()

    drain(xt.at[0:3], t_send)
    for a in range(2):
        drain(rows_of(a, 0, r + (line - 1) * (r - across[a])), w_send.at[2, a])
        for i in range(line):
            @pl.when(z == i)
            def _():
                if i < line - 1:
                    drain(rows_of(a, 0, (i + 1) * (r + across[a])), w_send.at[0, a])
                if i > 0:
                    drain(rows_of(a, 0, (line - i) * (r + across[a])), w_send.at[1, a])
    drain(part.at[0:nb], a_send)
    drain(pbuf, b_send)
    drain(psum, c_send)


END = (
    ((0, 0, 0), ((2, 0),)), ((0, 0, 1), ()),
    ((1, 0, 0), ((2, 1),)), ((1, 1, 0), ()),
    ((2, 0, 0), ((2, 2), (2, 3), (0, "fill"))),
    ((1, 0, 1), ((1, "two"),)), ((1, 1, 1), ()), ((2, 1, 0), ()),
    ((2, 0, 1), ((2, "two"),)), ((2, 1, 1), ((3, 0),)),
    ((0, 1, 0), ()), ((0, 1, 1), ((3, 1),)), ((3, 0, 0), ()),
    ((3, 1, 0), ((3, 2), (3, 3))), ((3, 0, 1), ((3, "two"),)), ((3, 1, 1), ()),
)
INNER = (
    ((0, 0, 0), ((1, "two"), (0, "own two"))), ((0, 0, 1), ()),
    ((1, 0, 0), ()), ((1, 0, 1), ()),
    ((2, 0, 0), ((2, "two"), (0, "own"))), ((2, 0, 1), ()),
    ((0, 1, 0), ((3, 0), (3, 1))), ((0, 1, 1), ((3, 2),)),
    ((1, 1, 0), ((3, 3),)), ((1, 1, 1), ()),
    ((3, 0, 0), ((3, "two"),)), ((3, 0, 1), ()),
    ((2, 1, 0), ()), ((2, 1, 1), ()), ((3, 1, 0), ()), ((3, 1, 1), ()),
)
EARLY = (0, 1)
BETWEEN = (2, 3)
FILL = ((), (0, 1), (2, 3))


def cut(r, share):
    across = r * share // 32 // 8 * 8
    lead = (LANES - across) * 21 // 32 // 8 * 8
    h = LANES // 2
    return [(0, h), (h, h), (LANES, lead), (LANES + lead, LANES - across - lead), (r - across, across)]


def fused(n_fs, prompt_tokens, norm_gain, up_master, down_master):
    T, dl = prompt_tokens.shape
    r, F = up_master.shape
    D = r * n_fs
    line = n_fs // 2
    pieces = (cut(r, 3), cut(r, 7))
    nblk, nb, half = D // LANES, dl // LANES, T // 2
    bf = jnp.bfloat16
    dma = pltpu.SemaphoreType.DMA
    vmem = pl.BlockSpec(memory_space=pltpu.VMEM)
    hbm = pl.BlockSpec(memory_space=pl.ANY)
    return pl.pallas_call(
        functools.partial(kernel, line, pieces),
        out_shape=(pltpu.VMEM((D, F), bf), pltpu.VMEM((D, F), bf), pltpu.VMEM((T, dl), bf)),
        in_specs=[hbm] * 4,
        out_specs=(vmem, vmem, vmem),
        scratch_shapes=[
            pltpu.VMEM((4, T, dl), bf), pltpu.VMEM((T, D), bf), pltpu.VMEM((T, F), bf),
            pltpu.VMEM((nblk, T, LANES), bf), pltpu.VMEM((2 * nb, half, LANES), bf),
            pltpu.VMEM((2 * nb, half, LANES), bf),
            pltpu.VMEM((nb, T, LANES), bf), pltpu.VMEM((nb, T, LANES), bf),
            dma((3, 2)), dma((2, line - 1, len(pieces[0]))), dma((2,)), dma, dma((line, r // LANES)),
            dma, dma((4,)),
            dma, dma((nb,)), dma, dma((2 * nb,)), dma, dma((nb,)),
            dma, pltpu.VMEM((r, F), jnp.float32), pltpu.VMEM((r, F), jnp.float32),
            pltpu.VMEM((1, r), jnp.float32), dma((len(pieces[0]) + 2,)),
        ],
        compiler_params=pltpu.CompilerParams(
            collective_id=0, has_side_effects=True, vmem_limit_bytes=55 * 2 ** 20),
    )(prompt_tokens, norm_gain.reshape(1, r), up_master, down_master)


def put(src_a, src_b, src_c, dst_a, dst_b, dst_c, sem):
    copies = []
    for src, dst in ((src_a, dst_a), (src_b, dst_b), (src_c, dst_c)):
        n = 4 if src is not src_c else 1
        rows = src.shape[0] // n
        for i in range(n):
            part = pl.ds(i * rows, rows)
            copies.append(pltpu.make_async_copy(
                src.at[part, :], dst.at[part, :], sem.at[len(copies)]))
    for c in copies:
        c.start()
    for c in copies:
        c.wait()


def written(*arrays):
    hbm = pl.BlockSpec(memory_space=pl.ANY)
    return pl.pallas_call(
        put,
        out_shape=tuple(pltpu.HBM(a.shape, a.dtype) for a in arrays),
        in_specs=[pl.BlockSpec(memory_space=pltpu.VMEM)] * 3,
        out_specs=(pl.BlockSpec(memory_space=pltpu.HBM),) * 3,
        scratch_shapes=[pltpu.SemaphoreType.DMA((9,))],
        compiler_params=pltpu.CompilerParams(vmem_limit_bytes=2 ** 20),
    )(*(pltpu.with_memory_space_constraint(a, pltpu.VMEM) for a in arrays))


def solution(mesh):
    n_fs, n_tp = mesh.shape["fs"], mesh.shape["tp"]

    def shards(prompt_tokens, norm_gain, up_master, down_master):
        T, dl = prompt_tokens.shape
        r = up_master.shape[0]
        fits = (n_tp == 4 and n_fs == 8 and r == 2 * LANES
                and dl % LANES == 0 and T % (2 * LANES) == 0 and r * n_fs == dl * n_tp)
        if not fits:
            return plain(prompt_tokens, norm_gain, up_master, down_master)
        return written(*fused(n_fs, prompt_tokens, norm_gain, up_master, down_master))

    return jax.shard_map(
        shards,
        mesh=mesh,
        in_specs=(P("fs", "tp"), P("fs"), P("fs", "tp"), P("fs", "tp")),
        out_specs=(P(None, "tp"), P(None, "tp"), P("fs", "tp")),
        check_vma=False,
    )
```

```python
import functools

import jax
import jax.numpy as jnp
from jax import lax
from jax.experimental import pallas as pl
from jax.experimental.pallas import tpu as pltpu
from jax.sharding import PartitionSpec as P

MESH = pl.DeviceIdType.MESH
LANES = 128


def plain(prompt_tokens, norm_gain, up_master, down_master):
    up_folded = (norm_gain[:, None] * up_master).astype(jnp.bfloat16)
    down_cast = down_master.astype(jnp.bfloat16)
    whole = lax.all_gather(prompt_tokens, "tp", axis=1, tiled=True)
    width = whole.shape[1]
    hidden_units = up_master.shape[1] * lax.axis_size("tp")
    wide = whole.astype(jnp.float32)
    normed = (wide * lax.rsqrt(jnp.mean(wide * wide, axis=1, keepdims=True) + 1e-05)).astype(
        jnp.bfloat16
    )
    contract = (((1,), (1,)), ((), ()))
    serve_up, serve_down = (
        lax.all_gather(up_folded, "fs", axis=0, tiled=True),
        lax.all_gather(down_cast, "fs", axis=0, tiled=True),
    )
    hidden = jnp.dot(normed, serve_up, preferred_element_type=jnp.float32)
    act = jnp.square(jax.nn.relu(hidden * width ** (-0.5))).astype(jnp.bfloat16)
    product = lax.dot_general(act, serve_down, contract, preferred_element_type=jnp.float32)
    partial_value = (product * hidden_units ** (-0.5)).astype(jnp.bfloat16)
    mixed = lax.psum_scatter(partial_value, "tp", scatter_dimension=1, tiled=True)
    return (serve_up, serve_down, mixed)


def kernel(line, pieces, tok, gain_hbm, up_hbm, down_hbm, wu, wd, mixed,
           xt, xn, act, part, pbuf, psum, rin_p, rin_y,
           w_send, z_recv, x_recv, xa_recv, xb_recv, t_send, t_recv,
           a_send, a_recv, b_send, b_recv, c_send, c_recv,
           l_sem, up, down, gain, d_sem):
    T, dl = tok.shape
    r, F = up_hbm.shape
    D = wu.shape[0]
    tp = lax.axis_index("tp")
    fs = lax.axis_index("fs")
    z, x = fs // 2, fs % 2
    core, chip = tp % 2, tp // 2
    partner = tp + 1 - 2 * core
    mirror = (tp + 2) % 4
    diag = (partner + 2) % 4
    has_up, has_dn = z < line - 1, z > 0
    inner = has_up & has_dn
    outer = jnp.logical_not(inner)
    low = z < line / 2
    high = jnp.logical_not(low)
    W = (wu, wd)
    nb = dl // LANES
    per = r // LANES
    half = T // 2
    zdev = ((fs + 2, tp), (fs - 2, tp), (fs + 1 - 2 * x, tp))

    barrier = pltpu.get_barrier_semaphore()

    def greet(dev):
        pl.semaphore_signal(barrier, inc=1, device_id=dev, device_id_type=MESH)

    greet(zdev[2])
    pl.when(has_up)(lambda: greet(zdev[0]))
    pl.when(has_dn)(lambda: greet(zdev[1]))
    for other in (mirror, diag, partner):
        greet((fs, other))

    parts = len(pieces[0])
    one, two = list(range(parts - 1)), parts - 1

    def lane_rows(i):
        return slice(i * LANES, (i + 1) * LANES)

    load_gain = pltpu.make_async_copy(gain_hbm, gain, d_sem.at[parts])
    def piece_rows(p):
        return slice(pieces[0][p][0], sum(pieces[0][p]))

    load_up = [pltpu.make_async_copy(up_hbm.at[piece_rows(p), :], up.at[piece_rows(p), :],
                                     d_sem.at[p]) for p in range(parts)]
    load_down = pltpu.make_async_copy(down_hbm, down, d_sem.at[parts + 1])
    own_tok = pltpu.make_async_copy(tok, xt.at[tp], l_sem)
    for load in [load_gain] + [load_up[p] for p in [two] + one] + [own_tok, load_down]:
        load.start()

    base = pl.multiple_of(fs * r, r)

    def gains(i):
        return jnp.transpose(jnp.broadcast_to(gain[:, lane_rows(i)], (LANES, LANES)))

    def fold(p):
        load_up[p].wait()
        at, size = pieces[0][p]
        g = column[at // LANES][at % LANES:at % LANES + size]
        for c in range(F // LANES):
            cols = lane_rows(c)
            wu[pl.ds(pl.multiple_of(base + at, 8), size), cols] = (
                g * up[at:at + size, cols]).astype(jnp.bfloat16)

    across = [pieces[a][two][1] for a in range(2)]

    def block_at(p):
        return pieces[1][p][0] // LANES

    def rows_of(a, first, size):
        return W[a].at[pl.ds(pl.multiple_of(first, 8), size), :]

    def remote(ref, send_sem, recv_sem, way):
        return pltpu.make_async_remote_copy(
            src_ref=ref, dst_ref=ref, send_sem=send_sem, recv_sem=recv_sem,
            device_id=zdev[way], device_id_type=MESH)

    def piece(a, s, p, way):
        if way < 2:
            recv = z_recv.at[a, (s // 2 - z + (2, 0)[way]) % line,
                             two + (s + x) % 2 if p == two else p]
        elif p == two:
            recv = x_recv.at[a]
        else:
            recv = xb_recv.at[s // 2, block_at(p)] if a else xa_recv
        return remote(rows_of(a, s * r + pieces[a][p][0], pieces[a][p][1]), w_send.at[way, a], recv, way)

    def tok_copy(src, k, to):
        return pltpu.make_async_remote_copy(
            src_ref=src, dst_ref=xt.at[k], send_sem=t_send, recv_sem=t_recv.at[k],
            device_id=(fs, to), device_id_type=MESH)

    def send_z(a, s, which, up_cond, dn_cond):
        for p in which:
            pl.when(up_cond)(lambda: piece(a, s, p, 0).start())
            pl.when(dn_cond)(lambda: piece(a, s, p, 1).start())

    def send_x(a, s, which):
        for p in which:
            piece(a, s, p, 2).start()

    xs = fs + 1 - 2 * x

    def near(i, k):
        return (abs(k - i), -k if i < line / 2 else k)

    def chip_of(k):
        return (2 * k * per // nb) // 2

    def pick(table):
        got = jnp.int32(0)
        for i in range(line):
            for y in range(2):
                got = got + jnp.where((z == i) & (chip == y), jnp.int32(table(i, y)), jnp.int32(0))
        return got

    order_a = [pick(lambda i, y: sorted(range(line), key=lambda k: near(i, k))[q])
               for q in range(line)]
    order_b = [pick(lambda i, y: sorted(range(line), key=lambda k: (
        k != i, chip_of(k) == y, near(i, k)))[q]) for q in range(line)]
    own_late = inner & (pick(lambda i, y: int(chip_of(i) == y)) == 1)

    def arrived(a, zz, p, first, size):
        remote(rows_of(a, first, size), w_send.at[0, a],
               z_recv.at[a, (zz - z + line - 1) % line, p], 0).wait_recv()

    def pass_one(a, zz, p):
        same = zz * 2 + x
        arrived(a, zz, p, same * r + pieces[a][p][0], pieces[a][p][1])
        send_z(a, same, [p], (zz < z) & has_up, (zz > z) & has_dn)
        send_x(a, same, [p])

    def pass_two(a, zz, sides=(0, 1)):
        for side in sides:
            s = zz * 2 + (1 - x if side else x)
            arrived(a, zz, two + side, s * r + pieces[a][two][0], across[a])
            send_z(a, s, [two], (zz < z) & has_up, (zz > z) & has_dn)

    def send_two(a, up_cond, dn_cond):
        for s in (fs, xs):
            send_z(a, s, [two], up_cond, dn_cond)

    def forward_tokens():
        tok_copy(xt.at[mirror], mirror, mirror).wait_recv()
        tok_copy(xt.at[mirror], mirror, partner).start()

    load_gain.wait()
    column = [gains(i) for i in range(per)]
    links = 4 + has_up.astype(jnp.int32) + has_dn.astype(jnp.int32)
    fold(two)
    fold(one[0])
    pl.semaphore_wait(barrier, links)
    send_x(0, fs, [two])
    for p in one:
        if p != one[0]:
            fold(p)
        send_z(0, fs, [p], has_up, has_dn)
        send_x(0, fs, [p])
    send_z(0, fs, [two], has_up, has_dn)
    own_tok.wait()
    tok_copy(xt.at[tp], tp, mirror).start()
    tok_copy(xt.at[tp], tp, partner).start()
    load_down.wait()
    wd[pl.ds(base, r), :] = down[...].astype(jnp.bfloat16)
    pl.when(inner)(lambda: send_x(1, fs, [two]))
    piece(0, xs, two, 2).wait_recv()
    send_z(0, xs, [two], has_up, has_dn)
    send_z(1, fs, one + [two], outer & has_up, outer & has_dn)
    ahead = jnp.logical_not(own_late)

    for idx in range(1, line):
        for p in one:
            pass_one(0, order_a[idx], p)
        if idx == line - 2:
            @pl.when(outer)
            def _():
                send_x(1, fs, [two])
                forward_tokens()
        if idx == line - 1:
            @pl.when(outer)
            def _():
                send_x(1, fs, FILL[0])

            @pl.when(inner)
            def _():
                send_x(1, fs, one)
                forward_tokens()
        pass_two(0, order_a[idx])
        if idx == line - 2:
            @pl.when(inner)
            def _():
                send_z(1, fs, one, low, high)
                piece(1, xs, two, 2).wait_recv()
                send_two(1, low, high)

    @pl.when(inner)
    def _():
        send_z(1, fs, one, ahead & high, ahead & low)

    @pl.when(outer)
    def _():
        piece(1, xs, two, 2).wait_recv()
        send_z(1, xs, [two], has_up, has_dn)

    tok_copy(xt.at[partner], partner, partner).wait_recv()
    tok_copy(xt.at[diag], diag, partner).wait_recv()
    block = 64

    def norm(i, carry):
        rows = pl.ds(pl.multiple_of(i * block, block), block)
        wide = [xt[k, rows, :].astype(jnp.float32) for k in range(4)]
        sq = wide[0] * wide[0]
        for k in range(1, 4):
            sq = sq + wide[k] * wide[k]
        inv = lax.rsqrt(jnp.sum(sq, axis=1, keepdims=True) * (1.0 / D) + 1e-05)
        for k in range(4):
            xn[rows, k * dl:(k + 1) * dl] = (wide[k] * inv).astype(jnp.bfloat16)
        return carry

    lax.fori_loop(0, T // block, norm, 0)

    for p in one:
        pass_one(1, order_b[1], p)

    @pl.when(outer)
    def _():
        send_x(1, fs, FILL[1])

    @pl.when(inner)
    def _():
        for p in EARLY:
            pass_one(1, order_b[2], p)

    remote(rows_of(0, 0, line * (r - across[0])), w_send.at[2, 0], xa_recv, 2).wait_recv()

    mrows = 2 * LANES

    def first(i, carry):
        rows = pl.ds(pl.multiple_of(i * mrows, mrows), mrows)
        hidden = jnp.dot(xn[rows, :], wu[...], preferred_element_type=jnp.float32) * D ** (-0.5)
        hidden = jnp.maximum(hidden, 0.0)
        act[rows, :] = (hidden * hidden).astype(jnp.bfloat16)
        for k, p in enumerate(BETWEEN):
            pl.when(inner & (i == min(k, T // mrows - 1)))(lambda: pass_one(1, order_b[2], p))
        return carry

    lax.fori_loop(0, T // mrows, first, 0)

    scale = (F * 4) ** (-0.5)
    mine = pl.ds(pl.multiple_of(core * half, half), half)
    theirs = pl.ds(pl.multiple_of((1 - core) * half, half), half)
    total = line * 2 * per

    keeper = outer & (2 * z * per // nb == tp)
    roles = ((outer & jnp.logical_not(keeper), END), (keeper, KEEPER), (inner, INNER))
    codes = []
    for n in range(total):
        code = jnp.int32(0)
        for here, table in roles:
            q, side, h = table[n][0]
            s = order_b[q] * 2 + (x if side == 0 else 1 - x)
            code = code + jnp.where(here, (s * per + h) * 2 + side, jnp.int32(0))
        codes.append(code)

    def code_of(n):
        got = jnp.int32(0)
        for i in range(total):
            got = got + jnp.where(n == i, codes[i], jnp.int32(0))
        return got

    def owner_of(b):
        o = b // nb
        return o, (o // 2) == chip

    away = 2 * nb

    def to_partner(b):
        return pltpu.make_async_remote_copy(
            src_ref=part.at[b], dst_ref=rin_p.at[b % nb], send_sem=a_send,
            recv_sem=a_recv.at[b % nb], device_id=(fs, partner), device_id_type=MESH)

    def swap(b):
        return pltpu.make_async_remote_copy(
            src_ref=part.at[b, theirs, :], dst_ref=pbuf.at[b % away], send_sem=b_send,
            recv_sem=b_recv.at[b % away], device_id=(fs, partner), device_id_type=MESH)

    def to_owner(b, o):
        return pltpu.make_async_remote_copy(
            src_ref=psum.at[b % away], dst_ref=rin_y.at[b % nb, mine, :], send_sem=c_send,
            recv_sem=c_recv.at[b % nb], device_id=(fs, o), device_id_type=MESH)

    def second_half(b):
        o, here = owner_of(b)

        @pl.when(jnp.logical_not(here))
        def _():
            swap(b).wait_recv()
            psum[b % away] = (part[b, mine, :].astype(jnp.float32)
                              + pbuf[b % away].astype(jnp.float32)).astype(jnp.bfloat16)
            to_owner(b, o).start()

    def event(q, what):
        if what == "two":
            pass_two(1, order_b[q])
        elif what == "same":
            pass_two(1, order_b[q], (0,))
        elif what == "cross":
            pass_two(1, order_b[q], (1,))
        elif what == "fill":
            send_x(1, fs, q)
        elif what == "own":
            send_z(1, fs, one, own_late & high, own_late & low)
            send_two(1, own_late & high, own_late & low)
        elif what == "own two":
            send_two(1, ahead & high, ahead & low)
        else:
            pass_one(1, order_b[q], what)

    def body(n, carry):
        for here, table in roles:
            @pl.when(here)
            def _():
                for at in range(total):
                    if table[at][1]:
                        @pl.when(n == at)
                        def _():
                            for q, what in table[at][1]:
                                event(q, what)

        code = code_of(n)
        b, side = code // 2, code % 2
        s, h = b // per, b % per

        @pl.when(side == 1)
        def _():
            for i in range(per):
                size = sum(pieces[1][p][1] for p in one if block_at(p) == i)
                pl.when(h == i)(lambda: remote(
                    rows_of(1, s * r + i * LANES, size), w_send.at[2, 1],
                    xb_recv.at[s // 2, i], 2).wait_recv())

        rhs = wd[pl.ds(pl.multiple_of(b * LANES, LANES), LANES), :]
        product = lax.dot_general(act[...], rhs, (((1,), (1,)), ((), ())),
                                  preferred_element_type=jnp.float32)
        part[b] = (product * scale).astype(jnp.bfloat16)
        o, here = owner_of(b)

        @pl.when(here & (o != tp))
        def _():
            to_partner(b).start()

        @pl.when(jnp.logical_not(here))
        def _():
            swap(b).start()

        @pl.when(n > 0)
        def _():
            second_half(code_of(n - 1) // 2)

        return carry

    lax.fori_loop(0, total, body, 0)
    second_half(codes[total - 1] // 2)

    runs = nb // per if nb % per == 0 else 1
    for q in range(nb):
        i = (q % runs + x) % runs * (nb // runs) + q // runs
        b = tp * nb + i
        to_partner(b).wait_recv()
        pltpu.make_async_remote_copy(
            src_ref=part.at[b], dst_ref=rin_y.at[i], send_sem=c_send, recv_sem=c_recv.at[i],
            device_id=(fs, partner), device_id_type=MESH).wait_recv()
        mixed[:, pl.ds(pl.multiple_of(i * LANES, LANES), LANES)] = (
            part[b].astype(jnp.float32) + rin_p[i].astype(jnp.float32)
            + rin_y[i].astype(jnp.float32)).astype(jnp.bfloat16)

    def drain(ref, sem):
        pltpu.make_async_remote_copy(
            src_ref=ref, dst_ref=ref, send_sem=sem, recv_sem=l_sem,
            device_id=(fs, partner), device_id_type=MESH).wait_send()

    drain(xt.at[0:3], t_send)
    for a in range(2):
        drain(rows_of(a, 0, r + (line - 1) * (r - across[a])), w_send.at[2, a])
        for i in range(line):
            @pl.when(z == i)
            def _():
                if i < line - 1:
                    drain(rows_of(a, 0, (i + 1) * (r + across[a])), w_send.at[0, a])
                if i > 0:
                    drain(rows_of(a, 0, (line - i) * (r + across[a])), w_send.at[1, a])
    drain(part.at[0:nb], a_send)
    drain(pbuf, b_send)
    drain(psum, c_send)


END = (
    ((0, 0, 0), ((2, 0),)), ((0, 0, 1), ()),
    ((1, 0, 0), ((2, 1),)), ((1, 1, 0), ()),
    ((2, 0, 0), ((2, 2), (2, 3), ((2, 3), "fill"))),
    ((1, 0, 1), ((1, "two"),)), ((1, 1, 1), ()), ((2, 1, 0), ()),
    ((2, 0, 1), ((2, "two"),)), ((2, 1, 1), ((3, 0),)),
    ((0, 1, 0), ()), ((0, 1, 1), ((3, 1),)), ((3, 0, 0), ()),
    ((3, 1, 0), ((3, 2), (3, 3))), ((3, 0, 1), ((3, "same"),)), ((3, 1, 1), ((3, "cross"),)),
)
KEEPER = (
    ((0, 0, 0), ((2, 0),)), ((0, 0, 1), ()),
    ((1, 0, 0), ((2, 1),)), ((1, 1, 0), ()),
    ((2, 0, 0), ((2, 2), (2, 3), ((2,), "fill"))),
    ((1, 0, 1), ((1, "two"),)), ((1, 1, 1), ()), ((2, 1, 0), ()),
    ((2, 0, 1), ((2, "two"),)), ((2, 1, 1), ((3, 0),)),
    ((0, 1, 0), ()), ((3, 0, 0), ((3, 1),)),
    ((3, 1, 0), ((3, 2), (3, 3), ((3,), "fill"))), ((3, 0, 1), ((3, "same"),)), ((3, 1, 1), ((3, "cross"),)),
    ((0, 1, 1), ()),
)
INNER = (
    ((0, 0, 0), ((1, "two"), (0, "own two"))), ((0, 0, 1), ()),
    ((1, 0, 0), ()), ((1, 0, 1), ()),
    ((2, 0, 0), ((2, "two"), (0, "own"))), ((2, 0, 1), ()),
    ((0, 1, 0), ((3, 0), (3, 1))), ((0, 1, 1), ((3, 2),)),
    ((1, 1, 0), ((3, 3),)), ((1, 1, 1), ()),
    ((3, 0, 0), ((3, "two"),)), ((3, 0, 1), ()),
    ((2, 1, 0), ()), ((2, 1, 1), ()), ((3, 1, 0), ()), ((3, 1, 1), ()),
)
EARLY = (0, 1)
BETWEEN = (2, 3)
FILL = ((), (0, 1), (2, 3))


def cut(r, share):
    across = r * share // 32 // 8 * 8
    lead = (LANES - across) * 21 // 32 // 8 * 8
    h = LANES // 2
    return [(0, h), (h, h), (LANES, lead), (LANES + lead, LANES - across - lead), (r - across, across)]


def fused(n_fs, prompt_tokens, norm_gain, up_master, down_master):
    T, dl = prompt_tokens.shape
    r, F = up_master.shape
    D = r * n_fs
    line = n_fs // 2
    pieces = (cut(r, 3), cut(r, 7))
    nblk, nb, half = D // LANES, dl // LANES, T // 2
    bf = jnp.bfloat16
    dma = pltpu.SemaphoreType.DMA
    vmem = pl.BlockSpec(memory_space=pltpu.VMEM)
    hbm = pl.BlockSpec(memory_space=pl.ANY)
    return pl.pallas_call(
        functools.partial(kernel, line, pieces),
        out_shape=(pltpu.VMEM((D, F), bf), pltpu.VMEM((D, F), bf), pltpu.VMEM((T, dl), bf)),
        in_specs=[hbm] * 4,
        out_specs=(vmem, vmem, vmem),
        scratch_shapes=[
            pltpu.VMEM((4, T, dl), bf), pltpu.VMEM((T, D), bf), pltpu.VMEM((T, F), bf),
            pltpu.VMEM((nblk, T, LANES), bf), pltpu.VMEM((2 * nb, half, LANES), bf),
            pltpu.VMEM((2 * nb, half, LANES), bf),
            pltpu.VMEM((nb, T, LANES), bf), pltpu.VMEM((nb, T, LANES), bf),
            dma((3, 2)), dma((2, line - 1, len(pieces[0]) + 1)), dma((2,)), dma, dma((line, r // LANES)),
            dma, dma((4,)),
            dma, dma((nb,)), dma, dma((2 * nb,)), dma, dma((nb,)),
            dma, pltpu.VMEM((r, F), jnp.float32), pltpu.VMEM((r, F), jnp.float32),
            pltpu.VMEM((1, r), jnp.float32), dma((len(pieces[0]) + 2,)),
        ],
        compiler_params=pltpu.CompilerParams(
            collective_id=0, has_side_effects=True, vmem_limit_bytes=55 * 2 ** 20),
    )(prompt_tokens, norm_gain.reshape(1, r), up_master, down_master)


def put(src_a, src_b, src_c, dst_a, dst_b, dst_c, sem):
    copies = []
    for src, dst in ((src_a, dst_a), (src_b, dst_b), (src_c, dst_c)):
        n = 4 if src is not src_c else 1
        rows = src.shape[0] // n
        for i in range(n):
            part = pl.ds(i * rows, rows)
            copies.append(pltpu.make_async_copy(
                src.at[part, :], dst.at[part, :], sem.at[len(copies)]))
    for c in copies:
        c.start()
    for c in copies:
        c.wait()


def written(*arrays):
    hbm = pl.BlockSpec(memory_space=pl.ANY)
    return pl.pallas_call(
        put,
        out_shape=tuple(pltpu.HBM(a.shape, a.dtype) for a in arrays),
        in_specs=[pl.BlockSpec(memory_space=pltpu.VMEM)] * 3,
        out_specs=(pl.BlockSpec(memory_space=pltpu.HBM),) * 3,
        scratch_shapes=[pltpu.SemaphoreType.DMA((9,))],
        compiler_params=pltpu.CompilerParams(vmem_limit_bytes=2 ** 20),
    )(*(pltpu.with_memory_space_constraint(a, pltpu.VMEM) for a in arrays))


def solution(mesh):
    n_fs, n_tp = mesh.shape["fs"], mesh.shape["tp"]

    def shards(prompt_tokens, norm_gain, up_master, down_master):
        T, dl = prompt_tokens.shape
        r = up_master.shape[0]
        fits = (n_tp == 4 and n_fs == 8 and r == 2 * LANES
                and dl % LANES == 0 and T % (2 * LANES) == 0 and r * n_fs == dl * n_tp)
        if not fits:
            return plain(prompt_tokens, norm_gain, up_master, down_master)
        return written(*fused(n_fs, prompt_tokens, norm_gain, up_master, down_master))

    return jax.shard_map(
        shards,
        mesh=mesh,
        in_specs=(P("fs", "tp"), P("fs"), P("fs", "tp"), P("fs", "tp")),
        out_specs=(P(None, "tp"), P(None, "tp"), P("fs", "tp")),
        check_vma=False,
    )
```

```python
import functools

import jax
import jax.numpy as jnp
from jax import lax
from jax.experimental import pallas as pl
from jax.experimental.pallas import tpu as pltpu
from jax.sharding import PartitionSpec as P

MESH = pl.DeviceIdType.MESH
LANES = 128


def plain(prompt_tokens, norm_gain, up_master, down_master):
    up_folded = (norm_gain[:, None] * up_master).astype(jnp.bfloat16)
    down_cast = down_master.astype(jnp.bfloat16)
    whole = lax.all_gather(prompt_tokens, "tp", axis=1, tiled=True)
    width = whole.shape[1]
    hidden_units = up_master.shape[1] * lax.axis_size("tp")
    wide = whole.astype(jnp.float32)
    normed = (wide * lax.rsqrt(jnp.mean(wide * wide, axis=1, keepdims=True) + 1e-05)).astype(
        jnp.bfloat16
    )
    contract = (((1,), (1,)), ((), ()))
    serve_up, serve_down = (
        lax.all_gather(up_folded, "fs", axis=0, tiled=True),
        lax.all_gather(down_cast, "fs", axis=0, tiled=True),
    )
    hidden = jnp.dot(normed, serve_up, preferred_element_type=jnp.float32)
    act = jnp.square(jax.nn.relu(hidden * width ** (-0.5))).astype(jnp.bfloat16)
    product = lax.dot_general(act, serve_down, contract, preferred_element_type=jnp.float32)
    partial_value = (product * hidden_units ** (-0.5)).astype(jnp.bfloat16)
    mixed = lax.psum_scatter(partial_value, "tp", scatter_dimension=1, tiled=True)
    return (serve_up, serve_down, mixed)


def kernel(line, pieces, tok, gain_hbm, up_hbm, down_hbm, wu, wd, mixed,
           xt, xn, act, part, pbuf, psum, rin_p, rin_y,
           w_send, z_recv, x_recv, xa_recv, xb_recv, t_send, t_recv,
           a_send, a_recv, b_send, b_recv, c_send, c_recv,
           l_sem, up, down, gain, d_sem):
    T, dl = tok.shape
    r, F = up_hbm.shape
    D = wu.shape[0]
    tp = lax.axis_index("tp")
    fs = lax.axis_index("fs")
    z, x = fs // 2, fs % 2
    core, chip = tp % 2, tp // 2
    partner = tp + 1 - 2 * core
    mirror = (tp + 2) % 4
    diag = (partner + 2) % 4
    has_up, has_dn = z < line - 1, z > 0
    inner = has_up & has_dn
    outer = jnp.logical_not(inner)
    low = z < line / 2
    high = jnp.logical_not(low)
    W = (wu, wd)
    nb = dl // LANES
    per = r // LANES
    half = T // 2
    zdev = ((fs + 2, tp), (fs - 2, tp), (fs + 1 - 2 * x, tp))

    barrier = pltpu.get_barrier_semaphore()

    def greet(dev):
        pl.semaphore_signal(barrier, inc=1, device_id=dev, device_id_type=MESH)

    greet(zdev[2])
    pl.when(has_up)(lambda: greet(zdev[0]))
    pl.when(has_dn)(lambda: greet(zdev[1]))
    for other in (mirror, diag, partner):
        greet((fs, other))

    parts = len(pieces[0])
    one, two = list(range(parts - 1)), parts - 1

    def lane_rows(i):
        return slice(i * LANES, (i + 1) * LANES)

    load_gain = pltpu.make_async_copy(gain_hbm, gain, d_sem.at[1])
    load_up = pltpu.make_async_copy(up_hbm, up, d_sem.at[0])
    load_down = pltpu.make_async_copy(down_hbm, down, d_sem.at[2])
    own_tok = pltpu.make_async_copy(tok, xt.at[tp], l_sem)
    for load in (load_gain, load_up, own_tok, load_down):
        load.start()

    base = pl.multiple_of(fs * r, r)

    def gains(i):
        return jnp.transpose(jnp.broadcast_to(gain[:, lane_rows(i)], (LANES, LANES)))

    def fold(p):
        at, size = pieces[0][p]
        g = column[at // LANES][at % LANES:at % LANES + size]
        for c in range(F // LANES):
            cols = lane_rows(c)
            wu[pl.ds(pl.multiple_of(base + at, 8), size), cols] = (
                g * up[at:at + size, cols]).astype(jnp.bfloat16)

    across = [pieces[a][two][1] for a in range(2)]

    def block_at(p):
        return pieces[1][p][0] // LANES

    def rows_of(a, first, size):
        return W[a].at[pl.ds(pl.multiple_of(first, 8), size), :]

    def remote(ref, send_sem, recv_sem, way):
        return pltpu.make_async_remote_copy(
            src_ref=ref, dst_ref=ref, send_sem=send_sem, recv_sem=recv_sem,
            device_id=zdev[way], device_id_type=MESH)

    def piece(a, s, p, way):
        if way < 2:
            recv = z_recv.at[a, (s // 2 - z + (2, 0)[way]) % line,
                             two + (s + x) % 2 if p == two else p]
        elif p == two:
            recv = x_recv.at[a]
        else:
            recv = xb_recv.at[s // 2, block_at(p)] if a else xa_recv
        return remote(rows_of(a, s * r + pieces[a][p][0], pieces[a][p][1]), w_send.at[way, a], recv, way)

    def tok_copy(src, k, to):
        return pltpu.make_async_remote_copy(
            src_ref=src, dst_ref=xt.at[k], send_sem=t_send, recv_sem=t_recv.at[k],
            device_id=(fs, to), device_id_type=MESH)

    def send_z(a, s, which, up_cond, dn_cond):
        for p in which:
            pl.when(up_cond)(lambda: piece(a, s, p, 0).start())
            pl.when(dn_cond)(lambda: piece(a, s, p, 1).start())

    def send_x(a, s, which):
        for p in which:
            piece(a, s, p, 2).start()

    xs = fs + 1 - 2 * x

    def near(i, k):
        return (abs(k - i), -k if i < line / 2 else k)

    def chip_of(k):
        return (2 * k * per // nb) // 2

    def pick(table):
        got = jnp.int32(0)
        for i in range(line):
            for y in range(2):
                got = got + jnp.where((z == i) & (chip == y), jnp.int32(table(i, y)), jnp.int32(0))
        return got

    order_a = [pick(lambda i, y: sorted(range(line), key=lambda k: near(i, k))[q])
               for q in range(line)]
    order_b = [pick(lambda i, y: sorted(range(line), key=lambda k: (
        k != i, chip_of(k) == y, near(i, k)))[q]) for q in range(line)]
    own_late = inner & (pick(lambda i, y: int(chip_of(i) == y)) == 1)

    def arrived(a, zz, p, first, size):
        remote(rows_of(a, first, size), w_send.at[0, a],
               z_recv.at[a, (zz - z + line - 1) % line, p], 0).wait_recv()

    def pass_one(a, zz, p):
        same = zz * 2 + x
        arrived(a, zz, p, same * r + pieces[a][p][0], pieces[a][p][1])
        send_z(a, same, [p], (zz < z) & has_up, (zz > z) & has_dn)
        send_x(a, same, [p])

    def pass_two(a, zz, sides=(0, 1)):
        for side in sides:
            s = zz * 2 + (1 - x if side else x)
            arrived(a, zz, two + side, s * r + pieces[a][two][0], across[a])
            send_z(a, s, [two], (zz < z) & has_up, (zz > z) & has_dn)

    def send_two(a, up_cond, dn_cond):
        for s in (fs, xs):
            send_z(a, s, [two], up_cond, dn_cond)

    def forward_tokens():
        tok_copy(xt.at[mirror], mirror, mirror).wait_recv()
        tok_copy(xt.at[mirror], mirror, partner).start()

    load_gain.wait()
    column = [gains(i) for i in range(per)]
    load_up.wait()
    links = 4 + has_up.astype(jnp.int32) + has_dn.astype(jnp.int32)
    fold(two)
    fold(one[0])
    pl.semaphore_wait(barrier, links)
    send_x(0, fs, [two])
    for p in one:
        if p != one[0]:
            fold(p)
        send_z(0, fs, [p], has_up, has_dn)
        send_x(0, fs, [p])
    send_z(0, fs, [two], has_up, has_dn)
    own_tok.wait()
    tok_copy(xt.at[tp], tp, mirror).start()
    tok_copy(xt.at[tp], tp, partner).start()
    load_down.wait()
    wd[pl.ds(base, r), :] = down[...].astype(jnp.bfloat16)
    pl.when(inner)(lambda: send_x(1, fs, [two]))
    piece(0, xs, two, 2).wait_recv()
    send_z(0, xs, [two], has_up, has_dn)
    send_z(1, fs, one + [two], outer & has_up, outer & has_dn)
    ahead = jnp.logical_not(own_late)

    for idx in range(1, line):
        for p in one:
            pass_one(0, order_a[idx], p)
        if idx == line - 2:
            @pl.when(outer)
            def _():
                send_x(1, fs, [two])
                forward_tokens()
        if idx == line - 1:
            @pl.when(outer)
            def _():
                send_x(1, fs, FILL[0])

            @pl.when(inner)
            def _():
                send_x(1, fs, one)
                forward_tokens()
        pass_two(0, order_a[idx])
        if idx == line - 2:
            @pl.when(inner)
            def _():
                send_z(1, fs, one, low, high)
                piece(1, xs, two, 2).wait_recv()
                send_two(1, low, high)

    @pl.when(inner)
    def _():
        send_z(1, fs, one, ahead & high, ahead & low)

    @pl.when(outer)
    def _():
        piece(1, xs, two, 2).wait_recv()
        send_z(1, xs, [two], has_up, has_dn)

    tok_copy(xt.at[partner], partner, partner).wait_recv()
    tok_copy(xt.at[diag], diag, partner).wait_recv()
    block = 64

    def norm(i, carry):
        rows = pl.ds(pl.multiple_of(i * block, block), block)
        wide = [xt[k, rows, :].astype(jnp.float32) for k in range(4)]
        sq = wide[0] * wide[0]
        for k in range(1, 4):
            sq = sq + wide[k] * wide[k]
        inv = lax.rsqrt(jnp.sum(sq, axis=1, keepdims=True) * (1.0 / D) + 1e-05)
        for k in range(4):
            xn[rows, k * dl:(k + 1) * dl] = (wide[k] * inv).astype(jnp.bfloat16)
        return carry

    lax.fori_loop(0, T // block, norm, 0)

    for p in one:
        pass_one(1, order_b[1], p)

    @pl.when(outer)
    def _():
        send_x(1, fs, FILL[1])

    @pl.when(inner)
    def _():
        for p in EARLY:
            pass_one(1, order_b[2], p)

    remote(rows_of(0, 0, line * (r - across[0])), w_send.at[2, 0], xa_recv, 2).wait_recv()

    mrows = 2 * LANES

    def first(i, carry):
        rows = pl.ds(pl.multiple_of(i * mrows, mrows), mrows)
        hidden = jnp.dot(xn[rows, :], wu[...], preferred_element_type=jnp.float32) * D ** (-0.5)
        hidden = jnp.maximum(hidden, 0.0)
        act[rows, :] = (hidden * hidden).astype(jnp.bfloat16)
        for k, p in enumerate(BETWEEN):
            pl.when(inner & (i == min(k, T // mrows - 1)))(lambda: pass_one(1, order_b[2], p))
        return carry

    lax.fori_loop(0, T // mrows, first, 0)

    scale = (F * 4) ** (-0.5)
    mine = pl.ds(pl.multiple_of(core * half, half), half)
    theirs = pl.ds(pl.multiple_of((1 - core) * half, half), half)
    total = line * 2 * per

    keeper = outer & (2 * z * per // nb == tp)
    roles = ((outer & jnp.logical_not(keeper), END), (keeper, KEEPER), (inner, INNER))
    codes = []
    for n in range(total):
        code = jnp.int32(0)
        for here, table in roles:
            q, side, h = table[n][0]
            s = order_b[q] * 2 + (x if side == 0 else 1 - x)
            code = code + jnp.where(here, (s * per + h) * 2 + side, jnp.int32(0))
        codes.append(code)

    def code_of(n):
        got = jnp.int32(0)
        for i in range(total):
            got = got + jnp.where(n == i, codes[i], jnp.int32(0))
        return got

    def owner_of(b):
        o = b // nb
        return o, (o // 2) == chip

    away = 2 * nb

    def to_partner(b):
        return pltpu.make_async_remote_copy(
            src_ref=part.at[b], dst_ref=rin_p.at[b % nb], send_sem=a_send,
            recv_sem=a_recv.at[b % nb], device_id=(fs, partner), device_id_type=MESH)

    def swap(b):
        return pltpu.make_async_remote_copy(
            src_ref=part.at[b, theirs, :], dst_ref=pbuf.at[b % away], send_sem=b_send,
            recv_sem=b_recv.at[b % away], device_id=(fs, partner), device_id_type=MESH)

    def to_owner(b, o):
        return pltpu.make_async_remote_copy(
            src_ref=psum.at[b % away], dst_ref=rin_y.at[b % nb, mine, :], send_sem=c_send,
            recv_sem=c_recv.at[b % nb], device_id=(fs, o), device_id_type=MESH)

    def second_half(b):
        o, here = owner_of(b)

        @pl.when(jnp.logical_not(here))
        def _():
            swap(b).wait_recv()
            psum[b % away] = (part[b, mine, :].astype(jnp.float32)
                              + pbuf[b % away].astype(jnp.float32)).astype(jnp.bfloat16)
            to_owner(b, o).start()

    runs = nb // per if nb % per == 0 else 1

    def finish(q):
        i = (q % runs + x) % runs * (nb // runs) + q // runs
        b = tp * nb + i
        to_partner(b).wait_recv()
        pltpu.make_async_remote_copy(
            src_ref=part.at[b], dst_ref=rin_y.at[i], send_sem=c_send, recv_sem=c_recv.at[i],
            device_id=(fs, partner), device_id_type=MESH).wait_recv()
        mixed[:, pl.ds(pl.multiple_of(i * LANES, LANES), LANES)] = (
            part[b].astype(jnp.float32) + rin_p[i].astype(jnp.float32)
            + rin_y[i].astype(jnp.float32)).astype(jnp.bfloat16)

    def event(q, what):
        if what == "two":
            pass_two(1, order_b[q])
        elif what == "same":
            pass_two(1, order_b[q], (0,))
        elif what == "cross":
            pass_two(1, order_b[q], (1,))
        elif what == "fill":
            send_x(1, fs, q)
        elif what == "own":
            send_z(1, fs, one, own_late & high, own_late & low)
            send_two(1, own_late & high, own_late & low)
        elif what == "own two":
            send_two(1, ahead & high, ahead & low)
        else:
            pass_one(1, order_b[q], what)

    def body(n, carry):
        for here, table in roles:
            @pl.when(here)
            def _():
                for at in range(total):
                    if table[at][1]:
                        @pl.when(n == at)
                        def _():
                            for q, what in table[at][1]:
                                event(q, what)

        @pl.when(keeper & (n == total - 2))
        def _():
            for q in range(nb - 1):
                finish(q)

        code = code_of(n)
        b, side = code // 2, code % 2
        s, h = b // per, b % per

        @pl.when(side == 1)
        def _():
            for i in range(per):
                size = sum(pieces[1][p][1] for p in one if block_at(p) == i)
                pl.when(h == i)(lambda: remote(
                    rows_of(1, s * r + i * LANES, size), w_send.at[2, 1],
                    xb_recv.at[s // 2, i], 2).wait_recv())

        rhs = wd[pl.ds(pl.multiple_of(b * LANES, LANES), LANES), :]
        product = lax.dot_general(act[...], rhs, (((1,), (1,)), ((), ())),
                                  preferred_element_type=jnp.float32)
        part[b] = (product * scale).astype(jnp.bfloat16)
        o, here = owner_of(b)

        @pl.when(here & (o != tp))
        def _():
            to_partner(b).start()

        @pl.when(jnp.logical_not(here))
        def _():
            swap(b).start()

        @pl.when(n > 0)
        def _():
            second_half(code_of(n - 1) // 2)

        return carry

    lax.fori_loop(0, total, body, 0)
    second_half(codes[total - 1] // 2)

    @pl.when(jnp.logical_not(keeper))
    def _():
        for q in range(nb - 1):
            finish(q)

    finish(nb - 1)

    def drain(ref, sem):
        pltpu.make_async_remote_copy(
            src_ref=ref, dst_ref=ref, send_sem=sem, recv_sem=l_sem,
            device_id=(fs, partner), device_id_type=MESH).wait_send()

    drain(xt.at[0:3], t_send)
    for a in range(2):
        drain(rows_of(a, 0, r + (line - 1) * (r - across[a])), w_send.at[2, a])
        for i in range(line):
            @pl.when(z == i)
            def _():
                if i < line - 1:
                    drain(rows_of(a, 0, (i + 1) * (r + across[a])), w_send.at[0, a])
                if i > 0:
                    drain(rows_of(a, 0, (line - i) * (r + across[a])), w_send.at[1, a])
    drain(part.at[0:nb], a_send)
    drain(pbuf, b_send)
    drain(psum, c_send)


END = (
    ((0, 0, 0), ((2, 0),)), ((0, 0, 1), ()),
    ((1, 0, 0), ((2, 1),)), ((1, 1, 0), ()),
    ((2, 0, 0), ((2, 2), (2, 3), ((2, 3), "fill"))),
    ((1, 0, 1), ((1, "two"),)), ((1, 1, 1), ()), ((2, 1, 0), ()),
    ((2, 0, 1), ((2, "two"),)), ((2, 1, 1), ((3, 0),)),
    ((0, 1, 0), ()), ((0, 1, 1), ((3, 1),)), ((3, 0, 0), ()),
    ((3, 1, 0), ((3, 2), (3, 3))), ((3, 0, 1), ((3, "same"),)), ((3, 1, 1), ((3, "cross"),)),
)
KEEPER = (
    ((0, 0, 0), ((2, 0),)), ((0, 0, 1), ()),
    ((1, 0, 0), ((2, 1),)), ((1, 1, 0), ()),
    ((2, 0, 0), ((2, 2), (2, 3), ((2,), "fill"))),
    ((1, 0, 1), ((1, "two"),)), ((1, 1, 1), ()), ((2, 1, 0), ()),
    ((2, 0, 1), ((2, "two"),)), ((2, 1, 1), ((3, 0),)),
    ((0, 1, 0), ()), ((3, 0, 0), ((3, 1),)),
    ((3, 1, 0), ((3, 2), (3, 3), ((3,), "fill"))), ((3, 0, 1), ((3, "same"),)), ((3, 1, 1), ((3, "cross"),)),
    ((0, 1, 1), ()),
)
INNER = (
    ((0, 0, 0), ((1, "two"), (0, "own two"))), ((0, 0, 1), ()),
    ((1, 0, 0), ()), ((1, 0, 1), ()),
    ((2, 0, 0), ((2, "two"), (0, "own"))), ((2, 0, 1), ()),
    ((0, 1, 0), ((3, 0), (3, 1))), ((0, 1, 1), ((3, 2),)),
    ((1, 1, 0), ((3, 3),)), ((1, 1, 1), ()),
    ((3, 0, 0), ((3, "two"),)), ((3, 0, 1), ()),
    ((2, 1, 0), ()), ((2, 1, 1), ()), ((3, 1, 0), ()), ((3, 1, 1), ()),
)
EARLY = (0, 1)
BETWEEN = (2, 3)
FILL = ((), (0, 1), (2, 3))


def cut(r, share):
    across = r * share // 32 // 8 * 8
    lead = (LANES - across) * 21 // 32 // 8 * 8
    h = LANES // 2
    return [(0, h), (h, h), (LANES, lead), (LANES + lead, LANES - across - lead), (r - across, across)]


def fused(n_fs, prompt_tokens, norm_gain, up_master, down_master):
    T, dl = prompt_tokens.shape
    r, F = up_master.shape
    D = r * n_fs
    line = n_fs // 2
    pieces = (cut(r, 3), cut(r, 7))
    nblk, nb, half = D // LANES, dl // LANES, T // 2
    bf = jnp.bfloat16
    dma = pltpu.SemaphoreType.DMA
    vmem = pl.BlockSpec(memory_space=pltpu.VMEM)
    hbm = pl.BlockSpec(memory_space=pl.ANY)
    return pl.pallas_call(
        functools.partial(kernel, line, pieces),
        out_shape=(pltpu.VMEM((D, F), bf), pltpu.VMEM((D, F), bf), pltpu.VMEM((T, dl), bf)),
        in_specs=[hbm] * 4,
        out_specs=(vmem, vmem, vmem),
        scratch_shapes=[
            pltpu.VMEM((4, T, dl), bf), pltpu.VMEM((T, D), bf), pltpu.VMEM((T, F), bf),
            pltpu.VMEM((nblk, T, LANES), bf), pltpu.VMEM((2 * nb, half, LANES), bf),
            pltpu.VMEM((2 * nb, half, LANES), bf),
            pltpu.VMEM((nb, T, LANES), bf), pltpu.VMEM((nb, T, LANES), bf),
            dma((3, 2)), dma((2, line - 1, len(pieces[0]) + 1)), dma((2,)), dma, dma((line, r // LANES)),
            dma, dma((4,)),
            dma, dma((nb,)), dma, dma((2 * nb,)), dma, dma((nb,)),
            dma, pltpu.VMEM((r, F), jnp.float32), pltpu.VMEM((r, F), jnp.float32),
            pltpu.VMEM((1, r), jnp.float32), dma((3,)),
        ],
        compiler_params=pltpu.CompilerParams(
            collective_id=0, has_side_effects=True, vmem_limit_bytes=55 * 2 ** 20),
    )(prompt_tokens, norm_gain.reshape(1, r), up_master, down_master)


def put(src_a, src_b, src_c, dst_a, dst_b, dst_c, sem):
    copies = []
    for src, dst in ((src_a, dst_a), (src_b, dst_b), (src_c, dst_c)):
        n = 4 if src is not src_c else 1
        rows = src.shape[0] // n
        for i in range(n):
            part = pl.ds(i * rows, rows)
            copies.append(pltpu.make_async_copy(
                src.at[part, :], dst.at[part, :], sem.at[len(copies)]))
    for c in copies:
        c.start()
    for c in copies:
        c.wait()


def written(*arrays):
    hbm = pl.BlockSpec(memory_space=pl.ANY)
    return pl.pallas_call(
        put,
        out_shape=tuple(pltpu.HBM(a.shape, a.dtype) for a in arrays),
        in_specs=[pl.BlockSpec(memory_space=pltpu.VMEM)] * 3,
        out_specs=(pl.BlockSpec(memory_space=pltpu.HBM),) * 3,
        scratch_shapes=[pltpu.SemaphoreType.DMA((9,))],
        compiler_params=pltpu.CompilerParams(vmem_limit_bytes=2 ** 20),
    )(*(pltpu.with_memory_space_constraint(a, pltpu.VMEM) for a in arrays))


def solution(mesh):
    n_fs, n_tp = mesh.shape["fs"], mesh.shape["tp"]

    def shards(prompt_tokens, norm_gain, up_master, down_master):
        T, dl = prompt_tokens.shape
        r = up_master.shape[0]
        fits = (n_tp == 4 and n_fs == 8 and r == 2 * LANES
                and dl % LANES == 0 and T % (2 * LANES) == 0 and r * n_fs == dl * n_tp)
        if not fits:
            return plain(prompt_tokens, norm_gain, up_master, down_master)
        return written(*fused(n_fs, prompt_tokens, norm_gain, up_master, down_master))

    return jax.shard_map(
        shards,
        mesh=mesh,
        in_specs=(P("fs", "tp"), P("fs"), P("fs", "tp"), P("fs", "tp")),
        out_specs=(P(None, "tp"), P(None, "tp"), P("fs", "tp")),
        check_vma=False,
    )
```

```python
import functools

import jax
import jax.numpy as jnp
from jax import lax
from jax.experimental import pallas as pl
from jax.experimental.pallas import tpu as pltpu
from jax.sharding import PartitionSpec as P

MESH = pl.DeviceIdType.MESH
LANES = 128


def plain(prompt_tokens, norm_gain, up_master, down_master):
    up_folded = (norm_gain[:, None] * up_master).astype(jnp.bfloat16)
    down_cast = down_master.astype(jnp.bfloat16)
    whole = lax.all_gather(prompt_tokens, "tp", axis=1, tiled=True)
    width = whole.shape[1]
    hidden_units = up_master.shape[1] * lax.axis_size("tp")
    wide = whole.astype(jnp.float32)
    normed = (wide * lax.rsqrt(jnp.mean(wide * wide, axis=1, keepdims=True) + 1e-05)).astype(
        jnp.bfloat16
    )
    contract = (((1,), (1,)), ((), ()))
    serve_up, serve_down = (
        lax.all_gather(up_folded, "fs", axis=0, tiled=True),
        lax.all_gather(down_cast, "fs", axis=0, tiled=True),
    )
    hidden = jnp.dot(normed, serve_up, preferred_element_type=jnp.float32)
    act = jnp.square(jax.nn.relu(hidden * width ** (-0.5))).astype(jnp.bfloat16)
    product = lax.dot_general(act, serve_down, contract, preferred_element_type=jnp.float32)
    partial_value = (product * hidden_units ** (-0.5)).astype(jnp.bfloat16)
    mixed = lax.psum_scatter(partial_value, "tp", scatter_dimension=1, tiled=True)
    return (serve_up, serve_down, mixed)


def kernel(line, pieces, tok, gain_hbm, up_hbm, down_hbm, wu, wd, mixed,
           xt, xn, act, part, pbuf, psum, rin_p, rin_y,
           w_send, z_recv, x_recv, xa_recv, xb_recv, t_send, t_recv,
           a_send, a_recv, b_send, b_recv, c_send, c_recv,
           l_sem, up, down, gain, d_sem):
    T, dl = tok.shape
    r, F = up_hbm.shape
    D = wu.shape[0]
    tp = lax.axis_index("tp")
    fs = lax.axis_index("fs")
    z, x = fs // 2, fs % 2
    core, chip = tp % 2, tp // 2
    partner = tp + 1 - 2 * core
    mirror = (tp + 2) % 4
    diag = (partner + 2) % 4
    has_up, has_dn = z < line - 1, z > 0
    inner = has_up & has_dn
    outer = jnp.logical_not(inner)
    low = z < line / 2
    high = jnp.logical_not(low)
    W = (wu, wd)
    nb = dl // LANES
    per = r // LANES
    half = T // 2
    zdev = ((fs + 2, tp), (fs - 2, tp), (fs + 1 - 2 * x, tp))

    barrier = pltpu.get_barrier_semaphore()

    def greet(dev):
        pl.semaphore_signal(barrier, inc=1, device_id=dev, device_id_type=MESH)

    greet(zdev[2])
    pl.when(has_up)(lambda: greet(zdev[0]))
    pl.when(has_dn)(lambda: greet(zdev[1]))
    for other in (mirror, diag, partner):
        greet((fs, other))

    parts = len(pieces[0])
    one, two = list(range(parts - 1)), parts - 1

    def lane_rows(i):
        return slice(i * LANES, (i + 1) * LANES)

    load_gain = pltpu.make_async_copy(gain_hbm, gain, d_sem.at[1])
    load_up = pltpu.make_async_copy(up_hbm, up, d_sem.at[0])
    load_down = pltpu.make_async_copy(down_hbm, down, d_sem.at[2])
    own_tok = pltpu.make_async_copy(tok, xt.at[tp], l_sem)
    for load in (load_gain, load_up, own_tok, load_down):
        load.start()

    base = pl.multiple_of(fs * r, r)

    def gains(i):
        return jnp.transpose(jnp.broadcast_to(gain[:, lane_rows(i)], (LANES, LANES)))

    def fold(p):
        at, size = pieces[0][p]
        g = column[at // LANES][at % LANES:at % LANES + size]
        for c in range(F // LANES):
            cols = lane_rows(c)
            wu[pl.ds(pl.multiple_of(base + at, 8), size), cols] = (
                g * up[at:at + size, cols]).astype(jnp.bfloat16)

    across = [pieces[a][two][1] for a in range(2)]

    def block_at(p):
        return pieces[1][p][0] // LANES

    def rows_of(a, first, size):
        return W[a].at[pl.ds(pl.multiple_of(first, 8), size), :]

    def remote(ref, send_sem, recv_sem, way):
        return pltpu.make_async_remote_copy(
            src_ref=ref, dst_ref=ref, send_sem=send_sem, recv_sem=recv_sem,
            device_id=zdev[way], device_id_type=MESH)

    def piece(a, s, p, way):
        if way < 2:
            recv = z_recv.at[a, (s // 2 - z + (2, 0)[way]) % line,
                             two + (s + x) % 2 if p == two else p]
        elif p == two:
            recv = x_recv.at[a]
        else:
            recv = xb_recv.at[s // 2, block_at(p)] if a else xa_recv
        return remote(rows_of(a, s * r + pieces[a][p][0], pieces[a][p][1]), w_send.at[way, a], recv, way)

    def tok_copy(src, k, to):
        return pltpu.make_async_remote_copy(
            src_ref=src, dst_ref=xt.at[k], send_sem=t_send, recv_sem=t_recv.at[k],
            device_id=(fs, to), device_id_type=MESH)

    def send_z(a, s, which, up_cond, dn_cond):
        for p in which:
            pl.when(up_cond)(lambda: piece(a, s, p, 0).start())
            pl.when(dn_cond)(lambda: piece(a, s, p, 1).start())

    def send_x(a, s, which):
        for p in which:
            piece(a, s, p, 2).start()

    xs = fs + 1 - 2 * x

    def near(i, k):
        return (abs(k - i), -k if i < line / 2 else k)

    def chip_of(k):
        return (2 * k * per // nb) // 2

    def pick(table):
        got = jnp.int32(0)
        for i in range(line):
            for y in range(2):
                got = got + jnp.where((z == i) & (chip == y), jnp.int32(table(i, y)), jnp.int32(0))
        return got

    order_a = [pick(lambda i, y: sorted(range(line), key=lambda k: near(i, k))[q])
               for q in range(line)]
    order_b = [pick(lambda i, y: sorted(range(line), key=lambda k: (
        k != i, chip_of(k) == y, near(i, k)))[q]) for q in range(line)]
    own_late = inner & (pick(lambda i, y: int(chip_of(i) == y)) == 1)

    def arrived(a, zz, p, first, size):
        remote(rows_of(a, first, size), w_send.at[0, a],
               z_recv.at[a, (zz - z + line - 1) % line, p], 0).wait_recv()

    def pass_one(a, zz, p):
        same = zz * 2 + x
        arrived(a, zz, p, same * r + pieces[a][p][0], pieces[a][p][1])
        send_z(a, same, [p], (zz < z) & has_up, (zz > z) & has_dn)
        send_x(a, same, [p])

    def pass_two(a, zz, sides=(0, 1)):
        for side in sides:
            s = zz * 2 + (1 - x if side else x)
            arrived(a, zz, two + side, s * r + pieces[a][two][0], across[a])
            send_z(a, s, [two], (zz < z) & has_up, (zz > z) & has_dn)

    def send_two(a, up_cond, dn_cond):
        for s in (fs, xs):
            send_z(a, s, [two], up_cond, dn_cond)

    def forward_tokens():
        tok_copy(xt.at[mirror], mirror, mirror).wait_recv()
        tok_copy(xt.at[mirror], mirror, partner).start()

    load_gain.wait()
    column = [gains(i) for i in range(per)]
    load_up.wait()
    links = 4 + has_up.astype(jnp.int32) + has_dn.astype(jnp.int32)
    fold(two)
    fold(one[0])
    pl.semaphore_wait(barrier, links)
    send_x(0, fs, [two])
    for p in one:
        if p != one[0]:
            fold(p)
        send_z(0, fs, [p], has_up, has_dn)
        send_x(0, fs, [p])
    send_z(0, fs, [two], has_up, has_dn)
    own_tok.wait()
    tok_copy(xt.at[tp], tp, mirror).start()
    load_down.wait()
    wd[pl.ds(base, r), :] = down[...].astype(jnp.bfloat16)
    pl.when(inner)(lambda: send_x(1, fs, [two]))
    piece(0, xs, two, 2).wait_recv()
    send_z(0, xs, [two], has_up, has_dn)
    send_z(1, fs, one + [two], outer & has_up, outer & has_dn)
    tok_copy(xt.at[tp], tp, partner).start()
    ahead = jnp.logical_not(own_late)

    for idx in range(1, line):
        for p in one:
            pass_one(0, order_a[idx], p)
        if idx == line - 2:
            @pl.when(outer)
            def _():
                send_x(1, fs, [two])
                forward_tokens()
        if idx == line - 1:
            @pl.when(outer)
            def _():
                send_x(1, fs, FILL[0])

            @pl.when(inner)
            def _():
                send_x(1, fs, one)
                forward_tokens()
        pass_two(0, order_a[idx])
        if idx == line - 2:
            @pl.when(inner)
            def _():
                send_z(1, fs, one, low, high)
                piece(1, xs, two, 2).wait_recv()
                send_two(1, low, high)

    @pl.when(inner)
    def _():
        send_z(1, fs, one, ahead & high, ahead & low)

    @pl.when(outer)
    def _():
        piece(1, xs, two, 2).wait_recv()
        send_z(1, xs, [two], has_up, has_dn)

    tok_copy(xt.at[partner], partner, partner).wait_recv()
    tok_copy(xt.at[diag], diag, partner).wait_recv()
    block = 64

    def norm(i, carry):
        rows = pl.ds(pl.multiple_of(i * block, block), block)
        wide = [xt[k, rows, :].astype(jnp.float32) for k in range(4)]
        sq = wide[0] * wide[0]
        for k in range(1, 4):
            sq = sq + wide[k] * wide[k]
        inv = lax.rsqrt(jnp.sum(sq, axis=1, keepdims=True) * (1.0 / D) + 1e-05)
        for k in range(4):
            xn[rows, k * dl:(k + 1) * dl] = (wide[k] * inv).astype(jnp.bfloat16)
        return carry

    lax.fori_loop(0, T // block, norm, 0)

    for p in one:
        pass_one(1, order_b[1], p)

    @pl.when(outer)
    def _():
        send_x(1, fs, FILL[1])

    @pl.when(inner)
    def _():
        for p in EARLY:
            pass_one(1, order_b[2], p)

    remote(rows_of(0, 0, line * (r - across[0])), w_send.at[2, 0], xa_recv, 2).wait_recv()

    mrows = 2 * LANES

    def first(i, carry):
        rows = pl.ds(pl.multiple_of(i * mrows, mrows), mrows)
        hidden = jnp.dot(xn[rows, :], wu[...], preferred_element_type=jnp.float32) * D ** (-0.5)
        hidden = jnp.maximum(hidden, 0.0)
        act[rows, :] = (hidden * hidden).astype(jnp.bfloat16)
        for k, p in enumerate(BETWEEN):
            pl.when(inner & (i == min(k, T // mrows - 1)))(lambda: pass_one(1, order_b[2], p))
        return carry

    lax.fori_loop(0, T // mrows, first, 0)

    scale = (F * 4) ** (-0.5)
    mine = pl.ds(pl.multiple_of(core * half, half), half)
    theirs = pl.ds(pl.multiple_of((1 - core) * half, half), half)
    total = line * 2 * per

    keeper = outer & (2 * z * per // nb == tp)
    roles = ((outer & jnp.logical_not(keeper), END), (keeper, KEEPER), (inner, INNER))
    codes = []
    for n in range(total):
        code = jnp.int32(0)
        for here, table in roles:
            q, side, h = table[n][0]
            s = order_b[q] * 2 + (x if side == 0 else 1 - x)
            code = code + jnp.where(here, (s * per + h) * 2 + side, jnp.int32(0))
        codes.append(code)

    def code_of(n):
        got = jnp.int32(0)
        for i in range(total):
            got = got + jnp.where(n == i, codes[i], jnp.int32(0))
        return got

    def owner_of(b):
        o = b // nb
        return o, (o // 2) == chip

    away = 2 * nb

    def to_partner(b):
        return pltpu.make_async_remote_copy(
            src_ref=part.at[b], dst_ref=rin_p.at[b % nb], send_sem=a_send,
            recv_sem=a_recv.at[b % nb], device_id=(fs, partner), device_id_type=MESH)

    def swap(b):
        return pltpu.make_async_remote_copy(
            src_ref=part.at[b, theirs, :], dst_ref=pbuf.at[b % away], send_sem=b_send,
            recv_sem=b_recv.at[b % away], device_id=(fs, partner), device_id_type=MESH)

    def to_owner(b, o):
        return pltpu.make_async_remote_copy(
            src_ref=psum.at[b % away], dst_ref=rin_y.at[b % nb, mine, :], send_sem=c_send,
            recv_sem=c_recv.at[b % nb], device_id=(fs, o), device_id_type=MESH)

    def second_half(b):
        o, here = owner_of(b)

        @pl.when(jnp.logical_not(here))
        def _():
            swap(b).wait_recv()
            psum[b % away] = (part[b, mine, :].astype(jnp.float32)
                              + pbuf[b % away].astype(jnp.float32)).astype(jnp.bfloat16)
            to_owner(b, o).start()

    runs = nb // per if nb % per == 0 else 1

    def finish(q):
        i = (q % runs + x) % runs * (nb // runs) + q // runs
        b = tp * nb + i
        to_partner(b).wait_recv()
        pltpu.make_async_remote_copy(
            src_ref=part.at[b], dst_ref=rin_y.at[i], send_sem=c_send, recv_sem=c_recv.at[i],
            device_id=(fs, partner), device_id_type=MESH).wait_recv()
        mixed[:, pl.ds(pl.multiple_of(i * LANES, LANES), LANES)] = (
            part[b].astype(jnp.float32) + rin_p[i].astype(jnp.float32)
            + rin_y[i].astype(jnp.float32)).astype(jnp.bfloat16)

    def event(q, what):
        if what == "two":
            pass_two(1, order_b[q])
        elif what == "same":
            pass_two(1, order_b[q], (0,))
        elif what == "cross":
            pass_two(1, order_b[q], (1,))
        elif what == "fill":
            send_x(1, fs, q)
        elif what == "own":
            send_z(1, fs, one, own_late & high, own_late & low)
            send_two(1, own_late & high, own_late & low)
        elif what == "own two":
            send_two(1, ahead & high, ahead & low)
        else:
            pass_one(1, order_b[q], what)

    def body(n, carry):
        for here, table in roles:
            @pl.when(here)
            def _():
                for at in range(total):
                    if table[at][1]:
                        @pl.when(n == at)
                        def _():
                            for q, what in table[at][1]:
                                event(q, what)

        @pl.when(keeper & (n == total - 2))
        def _():
            for q in range(nb - 1):
                finish(q)

        code = code_of(n)
        b, side = code // 2, code % 2
        s, h = b // per, b % per

        @pl.when(side == 1)
        def _():
            for i in range(per):
                size = sum(pieces[1][p][1] for p in one if block_at(p) == i)
                pl.when(h == i)(lambda: remote(
                    rows_of(1, s * r + i * LANES, size), w_send.at[2, 1],
                    xb_recv.at[s // 2, i], 2).wait_recv())

        rhs = wd[pl.ds(pl.multiple_of(b * LANES, LANES), LANES), :]
        product = lax.dot_general(act[...], rhs, (((1,), (1,)), ((), ())),
                                  preferred_element_type=jnp.float32)
        part[b] = (product * scale).astype(jnp.bfloat16)
        o, here = owner_of(b)

        @pl.when(here & (o != tp))
        def _():
            to_partner(b).start()

        @pl.when(jnp.logical_not(here))
        def _():
            swap(b).start()

        @pl.when(n > 0)
        def _():
            second_half(code_of(n - 1) // 2)

        return carry

    lax.fori_loop(0, total, body, 0)
    second_half(codes[total - 1] // 2)

    @pl.when(jnp.logical_not(keeper))
    def _():
        for q in range(nb - 1):
            finish(q)

    finish(nb - 1)

    def drain(ref, sem):
        pltpu.make_async_remote_copy(
            src_ref=ref, dst_ref=ref, send_sem=sem, recv_sem=l_sem,
            device_id=(fs, partner), device_id_type=MESH).wait_send()

    drain(xt.at[0:3], t_send)
    for a in range(2):
        drain(rows_of(a, 0, r + (line - 1) * (r - across[a])), w_send.at[2, a])
        for i in range(line):
            @pl.when(z == i)
            def _():
                if i < line - 1:
                    drain(rows_of(a, 0, (i + 1) * (r + across[a])), w_send.at[0, a])
                if i > 0:
                    drain(rows_of(a, 0, (line - i) * (r + across[a])), w_send.at[1, a])
    drain(part.at[0:nb], a_send)
    drain(pbuf, b_send)
    drain(psum, c_send)


END = (
    ((0, 0, 0), ((2, 0),)), ((0, 0, 1), ()),
    ((1, 0, 0), ((2, 1),)), ((1, 1, 0), ()),
    ((2, 0, 0), ((2, 2), (2, 3), ((2, 3), "fill"))),
    ((1, 0, 1), ((1, "two"),)), ((1, 1, 1), ()), ((2, 1, 0), ()),
    ((2, 0, 1), ((2, "two"),)), ((2, 1, 1), ((3, 0),)),
    ((0, 1, 0), ()), ((0, 1, 1), ((3, 1),)), ((3, 0, 0), ()),
    ((3, 1, 0), ((3, 2), (3, 3))), ((3, 0, 1), ((3, "same"),)), ((3, 1, 1), ((3, "cross"),)),
)
KEEPER = (
    ((0, 0, 0), ((2, 0),)), ((0, 0, 1), ()),
    ((1, 0, 0), ((2, 1),)), ((1, 1, 0), ()),
    ((2, 0, 0), ((2, 2), (2, 3), ((2,), "fill"))),
    ((1, 0, 1), ((1, "two"),)), ((1, 1, 1), ()), ((2, 1, 0), ()),
    ((2, 0, 1), ((2, "two"),)), ((2, 1, 1), ((3, 0),)),
    ((0, 1, 0), ()), ((3, 0, 0), ((3, 1),)),
    ((3, 1, 0), ((3, 2), (3, 3), ((3,), "fill"))), ((3, 0, 1), ((3, "same"),)), ((3, 1, 1), ((3, "cross"),)),
    ((0, 1, 1), ()),
)
INNER = (
    ((0, 0, 0), ((1, "two"), (0, "own two"))), ((0, 0, 1), ()),
    ((1, 0, 0), ()), ((1, 0, 1), ()),
    ((2, 0, 0), ((2, "two"), (0, "own"))), ((2, 0, 1), ()),
    ((0, 1, 0), ((3, 0), (3, 1))), ((0, 1, 1), ((3, 2),)),
    ((1, 1, 0), ((3, 3),)), ((1, 1, 1), ()),
    ((3, 0, 0), ((3, "two"),)), ((3, 0, 1), ()),
    ((2, 1, 0), ()), ((2, 1, 1), ()), ((3, 1, 0), ()), ((3, 1, 1), ()),
)
EARLY = (0, 1)
BETWEEN = (2, 3)
FILL = ((), (0, 1), (2, 3))


def cut(r, share):
    across = r * share // 32 // 8 * 8
    lead = (LANES - across) * 21 // 32 // 8 * 8
    h = LANES // 2
    return [(0, h), (h, h), (LANES, lead), (LANES + lead, LANES - across - lead), (r - across, across)]


def fused(n_fs, prompt_tokens, norm_gain, up_master, down_master):
    T, dl = prompt_tokens.shape
    r, F = up_master.shape
    D = r * n_fs
    line = n_fs // 2
    pieces = (cut(r, 3), cut(r, 7))
    nblk, nb, half = D // LANES, dl // LANES, T // 2
    bf = jnp.bfloat16
    dma = pltpu.SemaphoreType.DMA
    vmem = pl.BlockSpec(memory_space=pltpu.VMEM)
    hbm = pl.BlockSpec(memory_space=pl.ANY)
    return pl.pallas_call(
        functools.partial(kernel, line, pieces),
        out_shape=(pltpu.VMEM((D, F), bf), pltpu.VMEM((D, F), bf), pltpu.VMEM((T, dl), bf)),
        in_specs=[hbm] * 4,
        out_specs=(vmem, vmem, vmem),
        scratch_shapes=[
            pltpu.VMEM((4, T, dl), bf), pltpu.VMEM((T, D), bf), pltpu.VMEM((T, F), bf),
            pltpu.VMEM((nblk, T, LANES), bf), pltpu.VMEM((2 * nb, half, LANES), bf),
            pltpu.VMEM((2 * nb, half, LANES), bf),
            pltpu.VMEM((nb, T, LANES), bf), pltpu.VMEM((nb, T, LANES), bf),
            dma((3, 2)), dma((2, line - 1, len(pieces[0]) + 1)), dma((2,)), dma, dma((line, r // LANES)),
            dma, dma((4,)),
            dma, dma((nb,)), dma, dma((2 * nb,)), dma, dma((nb,)),
            dma, pltpu.VMEM((r, F), jnp.float32), pltpu.VMEM((r, F), jnp.float32),
            pltpu.VMEM((1, r), jnp.float32), dma((3,)),
        ],
        compiler_params=pltpu.CompilerParams(
            collective_id=0, has_side_effects=True, vmem_limit_bytes=55 * 2 ** 20),
    )(prompt_tokens, norm_gain.reshape(1, r), up_master, down_master)


def put(src_a, src_b, src_c, dst_a, dst_b, dst_c, sem):
    copies = []
    for src, dst in ((src_a, dst_a), (src_b, dst_b), (src_c, dst_c)):
        n = 4 if src is not src_c else 1
        rows = src.shape[0] // n
        for i in range(n):
            part = pl.ds(i * rows, rows)
            copies.append(pltpu.make_async_copy(
                src.at[part, :], dst.at[part, :], sem.at[len(copies)]))
    for c in copies:
        c.start()
    for c in copies:
        c.wait()


def written(*arrays):
    hbm = pl.BlockSpec(memory_space=pl.ANY)
    return pl.pallas_call(
        put,
        out_shape=tuple(pltpu.HBM(a.shape, a.dtype) for a in arrays),
        in_specs=[pl.BlockSpec(memory_space=pltpu.VMEM)] * 3,
        out_specs=(pl.BlockSpec(memory_space=pltpu.HBM),) * 3,
        scratch_shapes=[pltpu.SemaphoreType.DMA((9,))],
        compiler_params=pltpu.CompilerParams(vmem_limit_bytes=2 ** 20),
    )(*(pltpu.with_memory_space_constraint(a, pltpu.VMEM) for a in arrays))


def solution(mesh):
    n_fs, n_tp = mesh.shape["fs"], mesh.shape["tp"]

    def shards(prompt_tokens, norm_gain, up_master, down_master):
        T, dl = prompt_tokens.shape
        r = up_master.shape[0]
        fits = (n_tp == 4 and n_fs == 8 and r == 2 * LANES
                and dl % LANES == 0 and T % (2 * LANES) == 0 and r * n_fs == dl * n_tp)
        if not fits:
            return plain(prompt_tokens, norm_gain, up_master, down_master)
        return written(*fused(n_fs, prompt_tokens, norm_gain, up_master, down_master))

    return jax.shard_map(
        shards,
        mesh=mesh,
        in_specs=(P("fs", "tp"), P("fs"), P("fs", "tp"), P("fs", "tp")),
        out_specs=(P(None, "tp"), P(None, "tp"), P("fs", "tp")),
        check_vma=False,
    )
```

```python
import functools

import jax
import jax.numpy as jnp
from jax import lax
from jax.experimental import pallas as pl
from jax.experimental.pallas import tpu as pltpu
from jax.sharding import PartitionSpec as P

MESH = pl.DeviceIdType.MESH
LANES = 128


def plain(prompt_tokens, norm_gain, up_master, down_master):
    up_folded = (norm_gain[:, None] * up_master).astype(jnp.bfloat16)
    down_cast = down_master.astype(jnp.bfloat16)
    whole = lax.all_gather(prompt_tokens, "tp", axis=1, tiled=True)
    width = whole.shape[1]
    hidden_units = up_master.shape[1] * lax.axis_size("tp")
    wide = whole.astype(jnp.float32)
    normed = (wide * lax.rsqrt(jnp.mean(wide * wide, axis=1, keepdims=True) + 1e-05)).astype(
        jnp.bfloat16
    )
    contract = (((1,), (1,)), ((), ()))
    serve_up, serve_down = (
        lax.all_gather(up_folded, "fs", axis=0, tiled=True),
        lax.all_gather(down_cast, "fs", axis=0, tiled=True),
    )
    hidden = jnp.dot(normed, serve_up, preferred_element_type=jnp.float32)
    act = jnp.square(jax.nn.relu(hidden * width ** (-0.5))).astype(jnp.bfloat16)
    product = lax.dot_general(act, serve_down, contract, preferred_element_type=jnp.float32)
    partial_value = (product * hidden_units ** (-0.5)).astype(jnp.bfloat16)
    mixed = lax.psum_scatter(partial_value, "tp", scatter_dimension=1, tiled=True)
    return (serve_up, serve_down, mixed)


def kernel(line, pieces, tok, gain_hbm, up_hbm, down_hbm, wu, wd, mixed,
           xt, xn, act, part, pbuf, psum, rin_p, rin_y,
           w_send, z_recv, x_recv, xa_recv, xb_recv, t_send, t_recv,
           a_send, a_recv, b_send, b_recv, c_send, c_recv,
           l_sem, up, down, gain, d_sem):
    T, dl = tok.shape
    r, F = up_hbm.shape
    D = wu.shape[0]
    tp = lax.axis_index("tp")
    fs = lax.axis_index("fs")
    z, x = fs // 2, fs % 2
    core, chip = tp % 2, tp // 2
    partner = tp + 1 - 2 * core
    mirror = (tp + 2) % 4
    diag = (partner + 2) % 4
    has_up, has_dn = z < line - 1, z > 0
    inner = has_up & has_dn
    outer = jnp.logical_not(inner)
    low = z < line / 2
    high = jnp.logical_not(low)
    W = (wu, wd)
    nb = dl // LANES
    per = r // LANES
    half = T // 2
    zdev = ((fs + 2, tp), (fs - 2, tp), (fs + 1 - 2 * x, tp))

    barrier = pltpu.get_barrier_semaphore()

    def greet(dev):
        pl.semaphore_signal(barrier, inc=1, device_id=dev, device_id_type=MESH)

    greet(zdev[2])
    pl.when(has_up)(lambda: greet(zdev[0]))
    pl.when(has_dn)(lambda: greet(zdev[1]))
    for other in (mirror, diag, partner):
        greet((fs, other))

    parts = len(pieces[0])
    one, two = list(range(parts - 1)), parts - 1

    def lane_rows(i):
        return slice(i * LANES, (i + 1) * LANES)

    load_gain = pltpu.make_async_copy(gain_hbm, gain, d_sem.at[1])
    load_up = pltpu.make_async_copy(up_hbm, up, d_sem.at[0])
    load_down = pltpu.make_async_copy(down_hbm, down, d_sem.at[2])
    own_tok = pltpu.make_async_copy(tok, xt.at[tp], l_sem)
    for load in (load_gain, load_up, own_tok, load_down):
        load.start()

    base = pl.multiple_of(fs * r, r)

    def gains(i):
        return jnp.transpose(jnp.broadcast_to(gain[:, lane_rows(i)], (LANES, LANES)))

    def fold(p):
        at, size = pieces[0][p]
        g = column[at // LANES][at % LANES:at % LANES + size]
        for c in range(F // LANES):
            cols = lane_rows(c)
            wu[pl.ds(pl.multiple_of(base + at, 8), size), cols] = (
                g * up[at:at + size, cols]).astype(jnp.bfloat16)

    across = [pieces[a][two][1] for a in range(2)]

    def block_at(p):
        return pieces[1][p][0] // LANES

    def rows_of(a, first, size):
        return W[a].at[pl.ds(pl.multiple_of(first, 8), size), :]

    def remote(ref, send_sem, recv_sem, way):
        return pltpu.make_async_remote_copy(
            src_ref=ref, dst_ref=ref, send_sem=send_sem, recv_sem=recv_sem,
            device_id=zdev[way], device_id_type=MESH)

    def piece(a, s, p, way):
        if way < 2:
            recv = z_recv.at[a, (s // 2 - z + (2, 0)[way]) % line,
                             two + (s + x) % 2 if p == two else p]
        elif p == two:
            recv = x_recv.at[a]
        else:
            recv = xb_recv.at[s // 2, block_at(p)] if a else xa_recv
        return remote(rows_of(a, s * r + pieces[a][p][0], pieces[a][p][1]), w_send.at[way, a], recv, way)

    def tok_copy(src, k, to):
        return pltpu.make_async_remote_copy(
            src_ref=src, dst_ref=xt.at[k], send_sem=t_send, recv_sem=t_recv.at[k],
            device_id=(fs, to), device_id_type=MESH)

    def send_z(a, s, which, up_cond, dn_cond):
        for p in which:
            pl.when(up_cond)(lambda: piece(a, s, p, 0).start())
            pl.when(dn_cond)(lambda: piece(a, s, p, 1).start())

    def send_x(a, s, which):
        for p in which:
            piece(a, s, p, 2).start()

    xs = fs + 1 - 2 * x

    def near(i, k):
        return (abs(k - i), -k if i < line / 2 else k)

    def chip_of(k):
        return (2 * k * per // nb) // 2

    def pick(table):
        got = jnp.int32(0)
        for i in range(line):
            for y in range(2):
                got = got + jnp.where((z == i) & (chip == y), jnp.int32(table(i, y)), jnp.int32(0))
        return got

    order_a = [pick(lambda i, y: sorted(range(line), key=lambda k: near(i, k))[q])
               for q in range(line)]
    order_b = [pick(lambda i, y: sorted(range(line), key=lambda k: (
        k != i, chip_of(k) == y, near(i, k)))[q]) for q in range(line)]
    own_late = inner & (pick(lambda i, y: int(chip_of(i) == y)) == 1)

    def arrived(a, zz, p, first, size):
        remote(rows_of(a, first, size), w_send.at[0, a],
               z_recv.at[a, (zz - z + line - 1) % line, p], 0).wait_recv()

    def pass_one(a, zz, p):
        same = zz * 2 + x
        arrived(a, zz, p, same * r + pieces[a][p][0], pieces[a][p][1])
        send_z(a, same, [p], (zz < z) & has_up, (zz > z) & has_dn)
        send_x(a, same, [p])

    def pass_two(a, zz, sides=(0, 1)):
        for side in sides:
            s = zz * 2 + (1 - x if side else x)
            arrived(a, zz, two + side, s * r + pieces[a][two][0], across[a])
            send_z(a, s, [two], (zz < z) & has_up, (zz > z) & has_dn)

    def send_two(a, up_cond, dn_cond):
        for s in (fs, xs):
            send_z(a, s, [two], up_cond, dn_cond)

    def forward_tokens():
        tok_copy(xt.at[mirror], mirror, mirror).wait_recv()
        tok_copy(xt.at[mirror], mirror, partner).start()

    load_gain.wait()
    column = [gains(i) for i in range(per)]
    load_up.wait()
    links = 4 + has_up.astype(jnp.int32) + has_dn.astype(jnp.int32)
    fold(two)
    fold(one[0])
    pl.semaphore_wait(barrier, links)
    send_x(0, fs, [two])
    for p in one:
        if p != one[0]:
            fold(p)
        send_z(0, fs, [p], has_up, has_dn)
        send_x(0, fs, [p])
    send_z(0, fs, [two], has_up, has_dn)
    own_tok.wait()
    tok_copy(xt.at[tp], tp, mirror).start()
    tok_copy(xt.at[tp], tp, partner).start()
    load_down.wait()
    wd[pl.ds(base, r), :] = down[...].astype(jnp.bfloat16)
    pl.when(inner)(lambda: send_x(1, fs, [two]))
    piece(0, xs, two, 2).wait_recv()
    send_z(0, xs, [two], has_up, has_dn)
    send_z(1, fs, one + [two], outer & has_up, outer & has_dn)
    ahead = jnp.logical_not(own_late)

    for idx in range(1, line):
        for p in one:
            pass_one(0, order_a[idx], p)
        if idx == line - 2:
            @pl.when(outer)
            def _():
                send_x(1, fs, [two])
                forward_tokens()
        if idx == line - 1:
            @pl.when(outer)
            def _():
                send_x(1, fs, FILL[0])

            @pl.when(inner)
            def _():
                send_x(1, fs, one)
                forward_tokens()
        pass_two(0, order_a[idx])
        if idx == line - 2:
            @pl.when(inner)
            def _():
                send_z(1, fs, one, low, high)
                piece(1, xs, two, 2).wait_recv()
                send_two(1, low, high)

    @pl.when(inner)
    def _():
        send_z(1, fs, one, ahead & high, ahead & low)

    @pl.when(outer)
    def _():
        piece(1, xs, two, 2).wait_recv()
        send_z(1, xs, [two], has_up, has_dn)

    tok_copy(xt.at[partner], partner, partner).wait_recv()
    tok_copy(xt.at[diag], diag, partner).wait_recv()
    block = 64

    def norm(i, carry):
        rows = pl.ds(pl.multiple_of(i * block, block), block)
        wide = [xt[k, rows, :].astype(jnp.float32) for k in range(4)]
        sq = wide[0] * wide[0]
        for k in range(1, 4):
            sq = sq + wide[k] * wide[k]
        inv = lax.rsqrt(jnp.sum(sq, axis=1, keepdims=True) * (1.0 / D) + 1e-05)
        for k in range(4):
            xn[rows, k * dl:(k + 1) * dl] = (wide[k] * inv).astype(jnp.bfloat16)
        return carry

    lax.fori_loop(0, T // block, norm, 0)

    for p in one:
        pass_one(1, order_b[1], p)

    @pl.when(outer)
    def _():
        send_x(1, fs, FILL[1])

    @pl.when(inner)
    def _():
        for p in EARLY:
            pass_one(1, order_b[2], p)

    remote(rows_of(0, 0, line * (r - across[0])), w_send.at[2, 0], xa_recv, 2).wait_recv()

    mrows = 2 * LANES

    def first(i, carry):
        rows = pl.ds(pl.multiple_of(i * mrows, mrows), mrows)
        hidden = jnp.dot(xn[rows, :], wu[...], preferred_element_type=jnp.float32) * D ** (-0.5)
        hidden = jnp.maximum(hidden, 0.0)
        act[rows, :] = (hidden * hidden).astype(jnp.bfloat16)
        for k, p in enumerate(BETWEEN):
            pl.when(inner & (i == min(k, T // mrows - 1)))(lambda: pass_one(1, order_b[2], p))
        return carry

    lax.fori_loop(0, T // mrows, first, 0)

    scale = (F * 4) ** (-0.5)
    mine = pl.ds(pl.multiple_of(core * half, half), half)
    theirs = pl.ds(pl.multiple_of((1 - core) * half, half), half)
    total = line * 2 * per

    keeper = outer & (2 * z * per // nb == tp)
    roles = ((outer & jnp.logical_not(keeper), END), (keeper, KEEPER), (inner, INNER))
    codes = []
    for n in range(total):
        code = jnp.int32(0)
        for here, table in roles:
            q, side, h = table[n][0]
            s = order_b[q] * 2 + (x if side == 0 else 1 - x)
            code = code + jnp.where(here, (s * per + h) * 2 + side, jnp.int32(0))
        codes.append(code)

    def code_of(n):
        got = jnp.int32(0)
        for i in range(total):
            got = got + jnp.where(n == i, codes[i], jnp.int32(0))
        return got

    def owner_of(b):
        o = b // nb
        return o, (o // 2) == chip

    away = 2 * nb

    def to_partner(b):
        return pltpu.make_async_remote_copy(
            src_ref=part.at[b], dst_ref=rin_p.at[b % nb], send_sem=a_send,
            recv_sem=a_recv.at[b % nb], device_id=(fs, partner), device_id_type=MESH)

    def swap(b):
        return pltpu.make_async_remote_copy(
            src_ref=part.at[b, theirs, :], dst_ref=pbuf.at[b % away], send_sem=b_send,
            recv_sem=b_recv.at[b % away], device_id=(fs, partner), device_id_type=MESH)

    def to_owner(b, o):
        return pltpu.make_async_remote_copy(
            src_ref=psum.at[b % away], dst_ref=rin_y.at[b % nb, mine, :], send_sem=c_send,
            recv_sem=c_recv.at[b % nb], device_id=(fs, o), device_id_type=MESH)

    def second_half(b):
        o, here = owner_of(b)

        @pl.when(jnp.logical_not(here))
        def _():
            swap(b).wait_recv()
            psum[b % away] = (part[b, mine, :].astype(jnp.float32)
                              + pbuf[b % away].astype(jnp.float32)).astype(jnp.bfloat16)
            to_owner(b, o).start()

    runs = nb // per if nb % per == 0 else 1

    def finish(q):
        i = (q % runs + x) % runs * (nb // runs) + q // runs
        b = tp * nb + i
        to_partner(b).wait_recv()
        pltpu.make_async_remote_copy(
            src_ref=part.at[b], dst_ref=rin_y.at[i], send_sem=c_send, recv_sem=c_recv.at[i],
            device_id=(fs, partner), device_id_type=MESH).wait_recv()
        mixed[:, pl.ds(pl.multiple_of(i * LANES, LANES), LANES)] = (
            part[b].astype(jnp.float32) + rin_p[i].astype(jnp.float32)
            + rin_y[i].astype(jnp.float32)).astype(jnp.bfloat16)

    def event(q, what):
        if what == "two":
            pass_two(1, order_b[q])
        elif what == "same":
            pass_two(1, order_b[q], (0,))
        elif what == "cross":
            pass_two(1, order_b[q], (1,))
        elif what == "fill":
            send_x(1, fs, q)
        elif what == "own":
            send_z(1, fs, one, own_late & high, own_late & low)
            send_two(1, own_late & high, own_late & low)
        elif what == "own two":
            send_two(1, ahead & high, ahead & low)
        else:
            pass_one(1, order_b[q], what)

    def body(n, carry):
        for here, table in roles:
            @pl.when(here)
            def _():
                for at in range(total):
                    if table[at][1]:
                        @pl.when(n == at)
                        def _():
                            for q, what in table[at][1]:
                                event(q, what)

        @pl.when(keeper & (n == total - 2))
        def _():
            for q in range(nb - 1):
                finish(q)

        code = code_of(n)
        b, side = code // 2, code % 2
        s, h = b // per, b % per

        @pl.when(side == 1)
        def _():
            for i in range(per):
                size = sum(pieces[1][p][1] for p in one if block_at(p) == i)
                pl.when(h == i)(lambda: remote(
                    rows_of(1, s * r + i * LANES, size), w_send.at[2, 1],
                    xb_recv.at[s // 2, i], 2).wait_recv())

        rhs = wd[pl.ds(pl.multiple_of(b * LANES, LANES), LANES), :]
        product = lax.dot_general(act[...], rhs, (((1,), (1,)), ((), ())),
                                  preferred_element_type=jnp.float32)
        part[b] = (product * scale).astype(jnp.bfloat16)
        o, here = owner_of(b)

        @pl.when(here & (o != tp))
        def _():
            to_partner(b).start()

        @pl.when(jnp.logical_not(here))
        def _():
            swap(b).start()

        @pl.when(n > 0)
        def _():
            second_half(code_of(n - 1) // 2)

        return carry

    lax.fori_loop(0, total, body, 0)
    second_half(codes[total - 1] // 2)

    @pl.when(jnp.logical_not(keeper))
    def _():
        for q in range(nb - 1):
            finish(q)

    finish(nb - 1)

    def drain(ref, sem):
        pltpu.make_async_remote_copy(
            src_ref=ref, dst_ref=ref, send_sem=sem, recv_sem=l_sem,
            device_id=(fs, partner), device_id_type=MESH).wait_send()

    drain(xt.at[0:3], t_send)
    for a in range(2):
        drain(rows_of(a, 0, r + (line - 1) * (r - across[a])), w_send.at[2, a])
        for i in range(line):
            @pl.when(z == i)
            def _():
                if i < line - 1:
                    drain(rows_of(a, 0, (i + 1) * (r + across[a])), w_send.at[0, a])
                if i > 0:
                    drain(rows_of(a, 0, (line - i) * (r + across[a])), w_send.at[1, a])
    drain(part.at[0:nb], a_send)
    drain(pbuf, b_send)
    drain(psum, c_send)


END = (
    ((0, 0, 0), ((2, 0),)), ((0, 0, 1), ()),
    ((1, 0, 0), ((2, 1),)), ((1, 1, 0), ()),
    ((2, 0, 0), ((2, 2), (2, 3), ((2, 3), "fill"))),
    ((1, 0, 1), ((1, "two"),)), ((1, 1, 1), ()), ((2, 1, 0), ()),
    ((2, 0, 1), ((2, "two"),)), ((2, 1, 1), ((3, 0),)),
    ((0, 1, 0), ()), ((0, 1, 1), ((3, 1),)), ((3, 0, 0), ()),
    ((3, 1, 0), ((3, 2), (3, 3))), ((3, 0, 1), ((3, "same"),)), ((3, 1, 1), ((3, "cross"),)),
)
KEEPER = (
    ((0, 0, 0), ((2, 0),)), ((0, 0, 1), ()),
    ((1, 0, 0), ((2, 1),)), ((1, 1, 0), ()),
    ((2, 0, 0), ((2, 2), (2, 3), ((2,), "fill"))),
    ((1, 0, 1), ((1, "two"),)), ((1, 1, 1), ()), ((2, 1, 0), ()),
    ((2, 0, 1), ((2, "two"),)), ((2, 1, 1), ((3, 0),)),
    ((0, 1, 0), ()), ((3, 0, 0), ((3, 1),)),
    ((3, 1, 0), ((3, 2), (3, 3), ((3,), "fill"))), ((3, 0, 1), ((3, "same"),)), ((3, 1, 1), ((3, "cross"),)),
    ((0, 1, 1), ()),
)
INNER = (
    ((0, 0, 0), ((1, "two"), (0, "own two"))), ((0, 0, 1), ()),
    ((1, 0, 0), ()), ((1, 0, 1), ()),
    ((2, 0, 0), ((2, "two"), (0, "own"))), ((2, 0, 1), ()),
    ((0, 1, 0), ((3, 0), (3, 1))), ((0, 1, 1), ((3, 2),)),
    ((1, 1, 0), ((3, 3),)), ((1, 1, 1), ()),
    ((3, 0, 0), ((3, "two"),)), ((3, 0, 1), ()),
    ((2, 1, 0), ()), ((2, 1, 1), ()), ((3, 1, 0), ()), ((3, 1, 1), ()),
)
EARLY = (0, 1)
BETWEEN = (2, 3)
FILL = ((0,), (1,))


def cut(r, share):
    across = r * share // 32 // 8 * 8
    lead = (LANES - across) * 21 // 32 // 8 * 8
    h = LANES // 2
    return [(0, h), (h, h), (LANES, lead), (LANES + lead, LANES - across - lead), (r - across, across)]


def fused(n_fs, prompt_tokens, norm_gain, up_master, down_master):
    T, dl = prompt_tokens.shape
    r, F = up_master.shape
    D = r * n_fs
    line = n_fs // 2
    pieces = (cut(r, 3), cut(r, 7))
    nblk, nb, half = D // LANES, dl // LANES, T // 2
    bf = jnp.bfloat16
    dma = pltpu.SemaphoreType.DMA
    vmem = pl.BlockSpec(memory_space=pltpu.VMEM)
    hbm = pl.BlockSpec(memory_space=pl.ANY)
    return pl.pallas_call(
        functools.partial(kernel, line, pieces),
        out_shape=(pltpu.VMEM((D, F), bf), pltpu.VMEM((D, F), bf), pltpu.VMEM((T, dl), bf)),
        in_specs=[hbm] * 4,
        out_specs=(vmem, vmem, vmem),
        scratch_shapes=[
            pltpu.VMEM((4, T, dl), bf), pltpu.VMEM((T, D), bf), pltpu.VMEM((T, F), bf),
            pltpu.VMEM((nblk, T, LANES), bf), pltpu.VMEM((2 * nb, half, LANES), bf),
            pltpu.VMEM((2 * nb, half, LANES), bf),
            pltpu.VMEM((nb, T, LANES), bf), pltpu.VMEM((nb, T, LANES), bf),
            dma((3, 2)), dma((2, line - 1, len(pieces[0]) + 1)), dma((2,)), dma, dma((line, r // LANES)),
            dma, dma((4,)),
            dma, dma((nb,)), dma, dma((2 * nb,)), dma, dma((nb,)),
            dma, pltpu.VMEM((r, F), jnp.float32), pltpu.VMEM((r, F), jnp.float32),
            pltpu.VMEM((1, r), jnp.float32), dma((3,)),
        ],
        compiler_params=pltpu.CompilerParams(
            collective_id=0, has_side_effects=True, vmem_limit_bytes=55 * 2 ** 20),
    )(prompt_tokens, norm_gain.reshape(1, r), up_master, down_master)


def put(src_a, src_b, src_c, dst_a, dst_b, dst_c, sem):
    copies = []
    for src, dst in ((src_a, dst_a), (src_b, dst_b), (src_c, dst_c)):
        n = 4 if src is not src_c else 1
        rows = src.shape[0] // n
        for i in range(n):
            part = pl.ds(i * rows, rows)
            copies.append(pltpu.make_async_copy(
                src.at[part, :], dst.at[part, :], sem.at[len(copies)]))
    for c in copies:
        c.start()
    for c in copies:
        c.wait()


def written(*arrays):
    hbm = pl.BlockSpec(memory_space=pl.ANY)
    return pl.pallas_call(
        put,
        out_shape=tuple(pltpu.HBM(a.shape, a.dtype) for a in arrays),
        in_specs=[pl.BlockSpec(memory_space=pltpu.VMEM)] * 3,
        out_specs=(pl.BlockSpec(memory_space=pltpu.HBM),) * 3,
        scratch_shapes=[pltpu.SemaphoreType.DMA((9,))],
        compiler_params=pltpu.CompilerParams(vmem_limit_bytes=2 ** 20),
    )(*(pltpu.with_memory_space_constraint(a, pltpu.VMEM) for a in arrays))


def solution(mesh):
    n_fs, n_tp = mesh.shape["fs"], mesh.shape["tp"]

    def shards(prompt_tokens, norm_gain, up_master, down_master):
        T, dl = prompt_tokens.shape
        r = up_master.shape[0]
        fits = (n_tp == 4 and n_fs == 8 and r == 2 * LANES
                and dl % LANES == 0 and T % (2 * LANES) == 0 and r * n_fs == dl * n_tp)
        if not fits:
            return plain(prompt_tokens, norm_gain, up_master, down_master)
        return written(*fused(n_fs, prompt_tokens, norm_gain, up_master, down_master))

    return jax.shard_map(
        shards,
        mesh=mesh,
        in_specs=(P("fs", "tp"), P("fs"), P("fs", "tp"), P("fs", "tp")),
        out_specs=(P(None, "tp"), P(None, "tp"), P("fs", "tp")),
        check_vma=False,
    )
```
